32 devices in a mesh: ep: 16 (over z, x, core), tp: 2 (over y).
Axes of the slice: x: 2, y: 2, z: 4, core: 2. Of those that a mesh axis runs over, the one named last changes fastest.
Arguments:
- tokens: bfloat16 [2048, 2048], P('ep'), may hold values from -6 to 6
- routes: int32 [2048, 2], P('ep'), may hold values from 0 to 3, all different within a row; in each aligned block of 128 rows (0 to 127, 128 to 255, ...) at most 80 rows name the same one
- router_weight: bfloat16 [2048, 4], replicated, may hold values from -0.125 to 0.125
- gate_proj: bfloat16 [16, 2048, 1024], P('ep', None, 'tp'), may hold values from -0.125 to 0.125
- up_proj: bfloat16 [16, 2048, 1024], P('ep', None, 'tp'), may hold values from -0.125 to 0.125
- down_proj: bfloat16 [16, 1024, 2048], P('ep', 'tp'), may hold values from -0.09375 to 0.09375
- cotangent: bfloat16 [2048, 2048], P('ep'), may hold values from -1.5 to 1.5
Outputs:
- token_grad: bfloat16 [2048, 2048], P('ep', 'tp')
- gate_grad: float32 [2048, 2], P('ep')
- router_grad: float32 [2048, 4], P('ep')
- gate_proj_grad: float32 [16, 2048, 1024], P('ep', None, 'tp')
- up_proj_grad: float32 [16, 2048, 1024], P('ep', None, 'tp')
- down_proj_grad: float32 [16, 1024, 2048], P('ep', 'tp')
The draws below stay inside these ranges and needn't reach their ends.
Inputs may be any that keep to these rules, and one draw needn't show every extreme that they name: `routes`: each row names 2 different experts. Among the rows of one index of ep no expert is named more than 80 times, a bound that some block reaches.
All inputs are finite; a program needn't handle non-finite values.
Results may differ from the reference program's by a relative error of at most 0.0085.
Values may be sent and summed in bfloat16 or wider, within the bound.
A program may use at most 128 MiB of HBM per device.

```python
import math
import jax
import jax.numpy as jnp
import numpy as np
from jax import lax

D = 2048
FF = 4096
MEMBERS = 4
TOP = 2
TOK_DEV = 128
BLOCK_FF = 1024
EXPERTS = 4
CAP = 80
TOKENS = 2048
N_EP = 16


def levels(stream_key, shape, shards, smallest, top_value):
    factor_of = 1.0
    for axis_at, blocks in shards:
        steps = jax.random.uniform(jax.random.fold_in(jax.random.fold_in(stream_key, 6), axis_at), (blocks,), jnp.float32, smallest / len(shards), top_value / len(shards))
        factor_of = factor_of * jnp.repeat(jnp.exp(steps), shape[axis_at] // blocks).reshape((-1,) + (1,) * (len(shape) - 1 - axis_at))
    return factor_of


def routed_block(stream_key, own, number, rows, count, top, most, lean):
    order = jax.random.permutation(stream_key, count)
    packed, common = shares(count, rows * top, most, lean, True), shares(count, rows * top, most, lean, False)
    places = jnp.arange(count)

    def named(sizes, rotation):
        used = int((sizes > 0).sum())
        fixed = max(1, used // 4)
        moved = fixed + (places - fixed + rotation * (used - fixed)) % max(1, count - fixed)
        return jnp.zeros((count,), jnp.int32).at[order[jnp.where(places < fixed, places, moved)]].set(jnp.asarray(sizes, jnp.int32))

    sizes = jnp.where(number % 4 == 0, named(packed, number // 4), named(common, number - number // 4 - 1))
    mixed = jax.random.permutation(jax.random.fold_in(own, 3), count)
    donor, taker = mixed[0:count // 2 * 2:2], mixed[1:count // 2 * 2:2]
    slack = jnp.minimum(sizes[donor] - 1, most - sizes[taker]) // 2
    slack = jnp.where((donor == order[0]) | (taker == order[0]) | (sizes[taker] == 0), 0, jnp.maximum(slack, 0))
    moved = jax.random.randint(jax.random.fold_in(own, 4), (count // 2,), 0, 1 << 20) % (slack + 1)
    sizes = sizes.at[donor].add(-moved).at[taker].add(moved)
    items = jnp.searchsorted(jnp.cumsum(sizes), jnp.arange(rows * top), side="right").astype(jnp.int32)
    table = items.reshape(top, rows).T
    table = table[jax.random.permutation(jax.random.fold_in(own, 1), rows)]
    rotation = jax.random.randint(jax.random.fold_in(own, 2), (rows, 1), 0, top)
    return jnp.take_along_axis(table, (jnp.arange(top)[None, :] + rotation) % top, axis=1)


def shares(number_of, total, limit, slope, full):
    loads = [(1 << 20) // math.isqrt(rank ** slope) + 1 for rank in range(1, number_of + 1)]
    largest = limit if full else min(limit, max(-(-total // number_of), total * loads[0] // sum(loads)))
    least = 1 if total - largest >= number_of - 1 else 0
    holding, surplus = [largest] + [least] * (number_of - 1), total - largest - least * (number_of - 1)
    while surplus > 0:
        free = [i for i in range(1, number_of) if holding[i] < largest] or [i for i in range(1, number_of) if holding[i] < limit]
        pool, budget = sum([loads[i] for i in free]), surplus
        for i in free:
            addition = min(limit - holding[i], max(1, budget * loads[i] // pool), surplus)
            holding[i] = holding[i] + addition
            surplus = surplus - addition
    return np.array(holding)


def scatter_about(stream_key, shape, width, limit, pieces=(), held_as=jnp.bfloat16):
    result = width * jax.random.normal(stream_key, shape, jnp.float32)
    if pieces:
        result = result * levels(stream_key, shape, pieces, -0.22, 0.18)
    return jnp.clip(result, -limit, limit).astype(held_as)


def setup_inputs(seed: int = 0) -> dict:
    key_list = jax.random.split(jax.random.key(seed), 8)
    tokens = scatter_about(key_list[0], (TOKENS, D), 1.0, 6.0, ((0, 16),))
    routes_keys = jax.random.split(jax.random.fold_in(key_list[1], 1), TOKENS // TOK_DEV)
    routes_turns = jax.random.permutation(jax.random.fold_in(key_list[1], 3), TOKENS // TOK_DEV)
    routes = jax.vmap(lambda own, number: routed_block(jax.random.fold_in(key_list[1], 2), own, number, TOK_DEV, EXPERTS, TOP, CAP, 2))(routes_keys, routes_turns).reshape((TOKENS, TOP))
    router_weight = scatter_about(key_list[2], (D, EXPERTS), D ** -0.5, 0.125)
    gate_proj = scatter_about(key_list[3], (EXPERTS * MEMBERS, D, BLOCK_FF), D ** -0.5, 0.125, ((0, 16), (2, 2)))
    up_proj = scatter_about(key_list[4], (EXPERTS * MEMBERS, D, BLOCK_FF), D ** -0.5, 0.125, ((0, 16), (2, 2)))
    down_proj = scatter_about(key_list[5], (EXPERTS * MEMBERS, BLOCK_FF, D), FF ** -0.5, 0.09375, ((0, 16), (1, 2)))
    cotangent = scatter_about(key_list[6], (TOKENS, D), 0.25, 1.5, ((0, 16),))
    return dict(tokens=tokens, routes=routes, router_weight=router_weight, gate_proj=gate_proj, up_proj=up_proj, down_proj=down_proj, cotangent=cotangent)


def expert_backward(tok_rows, cot_rows, gate_rows, w_gate, w_up, w_down):
    gpre = jnp.dot(tok_rows, w_gate, preferred_element_type=jnp.float32)
    upre = jnp.dot(tok_rows, w_up, preferred_element_type=jnp.float32)
    sig = jax.nn.sigmoid(gpre)
    silu_val = gpre * sig
    hidden = (silu_val * upre).astype(jnp.bfloat16)
    qvals = lax.dot_general(cot_rows, w_down, (((1,), (1,)), ((), ())), preferred_element_type=jnp.float32)
    gate_part = jnp.sum(hidden.astype(jnp.float32) * qvals, axis=1)
    weight = gate_rows[:, None]
    dhid = weight * qvals
    d_gate = (dhid * upre * sig * (1.0 + gpre * (1.0 - sig))).astype(jnp.bfloat16)
    d_up = (dhid * silu_val).astype(jnp.bfloat16)
    scaled = (weight * hidden.astype(jnp.float32)).astype(jnp.bfloat16)
    grad_down = lax.dot_general(scaled, cot_rows, (((0,), (0,)), ((), ())), preferred_element_type=jnp.float32)
    grad_gate = lax.dot_general(tok_rows, d_gate, (((0,), (0,)), ((), ())), preferred_element_type=jnp.float32)
    grad_up = lax.dot_general(tok_rows, d_up, (((0,), (0,)), ((), ())), preferred_element_type=jnp.float32)
    row_grad = lax.dot_general(d_gate, w_gate, (((1,), (1,)), ((), ())), preferred_element_type=jnp.float32)
    row_grad = row_grad + lax.dot_general(d_up, w_up, (((1,), (1,)), ((), ())), preferred_element_type=jnp.float32)
    return grad_gate, grad_up, grad_down, row_grad, gate_part


def reference(tokens, routes, router_weight, gate_proj, up_proj, down_proj, cotangent):
    ntok = tokens.shape[0]
    experts = router_weight.shape[1]
    slots = N_EP * CAP
    logits = jnp.dot(tokens, router_weight, preferred_element_type=jnp.float32)
    onehot = (routes[:, :, None] == jnp.arange(experts, dtype=jnp.int32)[None, None, :]).astype(jnp.float32)
    chosen = jnp.sum(onehot * logits[:, None, :], axis=2)
    first = jax.nn.sigmoid(chosen[:, 0] - chosen[:, 1])
    gates = jnp.stack([first, 1.0 - first], axis=1)
    used = lax.optimization_barrier(gates.astype(jnp.bfloat16)).astype(jnp.float32)
    flat = onehot.reshape(N_EP, TOK_DEV * TOP, experts)
    rank = jnp.cumsum(flat, axis=1) - flat
    rank_sel = jnp.sum(flat * rank, axis=2).reshape(ntok, TOP).astype(jnp.int32)
    source = (jnp.arange(ntok, dtype=jnp.int32) // TOK_DEV)[:, None]
    target = routes * slots + source * CAP + rank_sel
    token_ids = jnp.broadcast_to(jnp.arange(ntok, dtype=jnp.int32)[:, None], (ntok, TOP))
    slot_token = jnp.full((experts * slots,), ntok, jnp.int32).at[target.reshape(-1)].set(token_ids.reshape(-1))
    slot_gate = jnp.zeros((experts * slots,), jnp.float32).at[target.reshape(-1)].set(used.reshape(-1))
    slot_token = slot_token.reshape(experts, slots)
    slot_gate = slot_gate.reshape(experts, slots)
    zero_row = jnp.zeros((1, D), jnp.bfloat16)
    pad_tok = jnp.concatenate([tokens, zero_row], axis=0)
    pad_cot = jnp.concatenate([cotangent, zero_row], axis=0)
    full_gate = gate_proj.reshape(experts, MEMBERS, D, BLOCK_FF).transpose(0, 2, 1, 3).reshape(experts, D, FF)
    full_up = up_proj.reshape(experts, MEMBERS, D, BLOCK_FF).transpose(0, 2, 1, 3).reshape(experts, D, FF)
    full_down = down_proj.reshape(experts, FF, D)

    def one_expert(items):
        ids, gate_rows, w_gate, w_up, w_down = items
        return expert_backward(pad_tok[ids], pad_cot[ids], gate_rows, w_gate, w_up, w_down)

    grad_gate, grad_up, grad_down, row_grads, gate_parts = lax.map(
        one_expert, (slot_token, slot_gate, full_gate, full_up, full_down))
    route_sum = jax.ops.segment_sum(row_grads.reshape(-1, D), slot_token.reshape(-1), num_segments=ntok + 1)[:ntok]
    gate_grad = gate_parts.reshape(-1)[target]
    delta = first * (1.0 - first) * (gate_grad[:, 0] - gate_grad[:, 1])
    dlogits = delta[:, None] * (onehot[:, 0] - onehot[:, 1])
    router_part = jnp.dot(dlogits, router_weight.astype(jnp.float32).T, precision=lax.Precision.HIGHEST)
    token_grad = (route_sum + router_part).astype(jnp.bfloat16)
    router_grad = jnp.dot(tokens.astype(jnp.float32).T, dlogits, precision=lax.Precision.HIGHEST)
    gate_proj_grad = grad_gate.reshape(experts, D, MEMBERS, BLOCK_FF).transpose(0, 2, 1, 3).reshape(experts * MEMBERS, D, BLOCK_FF)
    up_proj_grad = grad_up.reshape(experts, D, MEMBERS, BLOCK_FF).transpose(0, 2, 1, 3).reshape(experts * MEMBERS, D, BLOCK_FF)
    down_proj_grad = grad_down.reshape(experts * MEMBERS, BLOCK_FF, D)
    return token_grad, gate_grad, router_grad, gate_proj_grad, up_proj_grad, down_proj_grad
```

```python
import functools

import jax
import jax.numpy as jnp
from jax import lax
from jax.experimental import pallas as pl
from jax.experimental.pallas import tpu as pltpu
from jax.sharding import Mesh, PartitionSpec as P

MEMBERS = 4
TOP = 2
LANES = 128
F32 = jnp.float32
BF16 = jnp.bfloat16
MESH = pl.DeviceIdType.MESH
NT = (((1,), (1,)), ((), ()))


def rows_kernel(
    share, send_ref, tok_ref, slot_ref, oh_ref, first_ref, rw_ref, wg_hbm, wu_hbm, wd_hbm,
    x_hbm, dg_hbm, du_hbm, sc_hbm, grad_ref, gate_ref, router_ref,
    full, wg_ref, wu_ref, wd_ref, dg_ref, du_ref, sc_ref, back, core_in, xa_in, yb_in, ya_in, xb_in, home, place,
    gacc, gcore, gcore_in, gx_in, gt, gz, terms, terms_in,
    out_sem, hid_sem, send_sem, recv_sem, load_sem, gsend, grecv, tsend, trecv,
):
    experts, n_m, n_tp, capacity, _ = full.shape
    ntok, width = tok_ref.shape
    half = share // 2
    e, m, t = lax.axis_index("e"), lax.axis_index("m"), lax.axis_index("tp")
    n_ep = experts * n_m
    me = e * n_m + m
    x_half, core = lax.div(m, 2), lax.rem(m, 2)
    x_peer = lax.rem(m + 2, 4)
    core_peer = m + 1 - 2 * core
    held = n_m * capacity
    first_cols, last_cols = pl.ds(0, share), pl.ds(share, share + LANES)
    low, high = pl.ds(0, half), pl.ds(half, share - half)

    def ahead(j):
        return lax.rem(t + j, n_tp)

    def behind(j):
        return lax.rem(t + n_tp - j, n_tp)

    def ep_at(d):
        there = lax.rem(me + d, n_ep)
        return (lax.div(there, n_m), lax.rem(there, n_m), t)

    barrier = pltpu.get_barrier_semaphore()
    for d in range(1, n_ep):
        pl.semaphore_signal(barrier, inc=1, device_id=ep_at(d), device_id_type=MESH)
    for j in range(1, n_tp):
        pl.semaphore_signal(barrier, inc=1, device_id=(e, m, ahead(j)), device_id_type=MESH)
    loads = [
        pltpu.make_async_copy(src, dst, load_sem.at[n])
        for n, (src, dst) in enumerate(
            [(send_ref.at[e], full.at[0, m, t]), (wg_hbm, wg_ref), (wu_hbm, wu_ref), (wd_hbm, wd_ref)]
        )
    ]
    for load in loads:
        load.start()
    pl.semaphore_wait(barrier, n_ep - 1 + n_tp - 1)

    def remote(src, dst, kind, k, device):
        return pltpu.make_async_remote_copy(
            src_ref=src,
            dst_ref=dst,
            send_sem=send_sem.at[kind, k],
            recv_sem=recv_sem.at[kind, k],
            device_id=device,
            device_id_type=MESH,
        )

    def piece(k, src_m, src_t, cols=None):
        ref = full.at[k, src_m, src_t]
        return ref if cols is None else ref.at[:, cols]

    others = n_tp - 1
    X, CORE_OWN, CORE_X, Z, R1, R2A, R3B, RET = range(8)
    def y_kind(j): return 8 + (j - 1)
    def a_kind(j): return 8 + others + (j - 1)
    def b_kind(j): return 8 + 2 * others + (j - 1)
    def core_y(j): return 8 + 3 * others + (j - 1)
    def core_a(j): return 8 + 4 * others + (j - 1)
    def core_b(j): return 8 + 5 * others + (j - 1)
    def r2b(j): return 8 + 6 * others + (j - 1)
    def r3a(j): return 8 + 7 * others + (j - 1)

    x_to, core_to = (e, x_peer, t), (e, core_peer, t)

    def pass_on(ref, kind, k, device):
        remote(ref, ref, kind, k, device).start()

    def landed(ref, kind, k):
        remote(ref, ref, kind, k, core_to).wait_recv()

    def sent(ref, kind, k):
        remote(ref, ref, kind, k, core_to).wait_send()

    for k in range(1, experts):
        there = lax.rem(e + k, experts)
        remote(send_ref.at[there], full.at[k, m, t], Z, k, (there, m, t)).start()

    def own(k):
        mine = piece(k, m, t)
        @pl.when(k > 0)
        def _():
            landed(mine, Z, k)
            pass_on(mine, X, k, x_to)
            for j in range(1, n_tp):
                pass_on(mine, y_kind(j), k, (e, m, ahead(j)))
            pass_on(mine, CORE_OWN, k, core_to)

        @pl.when(k == 0)
        def _():
            src = send_ref.at[e]
            remote(src, mine, X, 0, x_to).start()
            for j in range(1, n_tp):
                remote(src, mine, y_kind(j), 0, (e, m, ahead(j))).start()
            remote(src, mine, CORE_OWN, 0, core_to).start()

    def neighbours(k):
        across = piece(k, x_peer, t)
        landed(across, X, k)
        for j in range(1, n_tp):
            pass_on(piece(k, x_peer, t, last_cols), b_kind(j), k, (e, m, ahead(j)))
        pass_on(across, CORE_X, k, core_to)
        for j in range(1, n_tp):
            beside = piece(k, m, behind(j))
            landed(beside, y_kind(j), k)
            pass_on(piece(k, m, behind(j), first_cols), a_kind(j), k, x_to)
            pass_on(beside, core_y(j), k, core_to)

    def corners(k):
        for j in range(1, n_tp):
            for cols, kind, across in ((first_cols, a_kind, core_a), (last_cols, b_kind, core_b)):
                ref = piece(k, x_peer, behind(j), cols)
                landed(ref, kind(j), k)
                pass_on(ref, across(j), k, core_to)

    other_x = lax.rem(core_peer + 2, 4)

    def partner(k):
        landed(piece(k, core_peer, t), CORE_OWN, k)
        landed(piece(k, other_x, t), CORE_X, k)
        for j in range(1, n_tp):
            landed(piece(k, core_peer, behind(j)), core_y(j), k)
            landed(piece(k, other_x, behind(j), first_cols), core_a(j), k)
            landed(piece(k, other_x, behind(j), last_cols), core_b(j), k)
        pltpu.make_async_copy(full.at[k], x_hbm.at[k], out_sem.at[k]).start()

    def hidden_copies(k):
        pairs = ((dg_ref, dg_hbm), (du_ref, du_hbm), (sc_ref, sc_hbm))
        return [pltpu.make_async_copy(a.at[k], b.at[k], hid_sem.at[n, k]) for n, (a, b) in enumerate(pairs)]

    def compute(k):
        def part(tp_at, base, size):
            return full[k, :, tp_at, :, base : base + size].reshape(held, size)

        def contract(base, w_ref, nt):
            total = None
            for tp_at in range(n_tp):
                cols = slice(tp_at * share, (tp_at + 1) * share)
                rows = part(tp_at, base, share)
                if nt:
                    term = lax.dot_general(rows, w_ref[0, :, cols], NT, preferred_element_type=F32)
                else:
                    term = jnp.dot(rows, w_ref[0, cols, :], preferred_element_type=F32)
                total = term if total is None else total + term
            return total

        gpre = contract(0, wg_ref, False)
        upre = contract(0, wu_ref, False)
        qvals = contract(share, wd_ref, True)
        extra = part(0, 2 * share, LANES).astype(F32)
        lane = lax.broadcasted_iota(jnp.int32, extra.shape, 1)
        weight = jnp.sum(jnp.where(lane == e, extra, 0.0), axis=1, keepdims=True)
        sig = jax.nn.sigmoid(gpre)
        silu_val = gpre * sig
        hidden = (silu_val * upre).astype(BF16).astype(F32)
        gate_part = jnp.sum(hidden * qvals, axis=1, keepdims=True)
        dhid = weight * qvals
        d_gate = (dhid * upre * sig * (1.0 + gpre * (1.0 - sig))).astype(BF16)
        d_up = (dhid * silu_val).astype(BF16)
        dg_ref[k] = d_gate
        du_ref[k] = d_up
        sc_ref[k] = (weight * hidden).astype(BF16)
        for copy in hidden_copies(k):
            copy.start()
        source = lax.rem(e + experts - k, experts)
        gate_lanes = jnp.where(lane == source, gate_part, 0.0).reshape(n_m, capacity, LANES)
        for at in range(n_m):
            gacc[at % 2, at // 2, :capacity, :] += gate_lanes[at]
        for tp_at in range(n_tp):
            cols = slice(tp_at * share, (tp_at + 1) * share)
            grad = lax.dot_general(d_gate, wg_ref[0, cols, :], NT, preferred_element_type=F32)
            grad = grad + lax.dot_general(d_up, wu_ref[0, cols, :], NT, preferred_element_type=F32)
            grad = grad.astype(BF16).reshape(n_m, capacity, share)
            for at in range(n_m):
                back[k, at % 2, at // 2, tp_at] = grad[at]
        remote(back.at[k, 1 - core], core_in.at[k], R1, k, core_to).start()

    def add(*terms):
        total = terms[0].astype(F32)
        for term in terms[1:]:
            total = total + term.astype(F32)
        return total.astype(BF16)

    x_other = 1 - x_half

    def across_a(k):
        return back.at[k, core, x_other, :, :, low]

    def across_b(k, j):
        return back.at[k, core, :, ahead(j), :, high]

    def reduce_first(k):
        landed(core_in.at[k], R1, k)
        back[k, core] = add(back[k, core], core_in[k])
        remote(across_a(k), xa_in.at[k], R2A, k, x_to).start()
        for j in range(1, n_tp):
            remote(across_b(k, j), yb_in.at[k, j - 1], r2b(j), k, (e, m, ahead(j))).start()

    def onward_a(k, j):
        return back.at[k, core, x_half, ahead(j), :, low]

    def onward_b(k):
        return back.at[k, core, x_other, t, :, high]

    def reduce_second(k):
        landed(xa_in.at[k], R2A, k)
        for j in range(1, n_tp):
            onward_a(k, j)[...] = add(onward_a(k, j)[...], xa_in[k, ahead(j)])
            remote(onward_a(k, j), ya_in.at[k, j - 1], r3a(j), k, (e, m, ahead(j))).start()
        for j in range(1, n_tp):
            landed(yb_in.at[k, j - 1], r2b(j), k)
        onward_b(k)[...] = add(onward_b(k)[...], *[yb_in[k, j - 1, x_other] for j in range(1, n_tp)])
        remote(onward_b(k), xb_in.at[k], R3B, k, x_to).start()

    def mine_back(k):
        return back.at[k, core, x_half, t]

    def reduce_third(k):
        for j in range(1, n_tp):
            landed(ya_in.at[k, j - 1], r3a(j), k)
        landed(xb_in.at[k], R3B, k)
        ref = mine_back(k)
        ref[:, :half] = add(ref[:, :half], xa_in[k, t], *[ya_in[k, j - 1] for j in range(1, n_tp)])
        ref[:, half:] = add(ref[:, half:], xb_in[k], *[yb_in[k, j - 1, x_half] for j in range(1, n_tp)])

        def away():
            there = lax.rem(e + experts - k, experts)
            remote(ref, home.at[e], RET, k, (there, m, t)).start()

        def here():
            home[e] = ref[...]

        if isinstance(k, int):
            (away if k else here)()
        else:
            pl.when(k > 0)(away)
            pl.when(k == 0)(here)

    gacc[...] = jnp.zeros_like(gacc)

    def step(i, carry):
        pl.when(i < experts)(lambda: own(i))
        pl.when((i >= 1) & (i < experts + 1))(lambda: neighbours(i - 1))
        pl.when(i >= 3)(lambda: reduce_first(i - 3))
        pl.when(i >= 4)(lambda: reduce_second(i - 4))
        pl.when(i >= 5)(lambda: reduce_third(i - 5))

        @pl.when(i == 2)
        def _():
            for load in loads:
                load.wait()

        @pl.when(i >= 2)
        def _():
            corners(i - 2)
            partner(i - 2)
            compute(i - 2)

        return carry

    lax.fori_loop(0, experts + 2, step, 0)

    def gate_copy(src, dst, n, device):
        return pltpu.make_async_remote_copy(
            src_ref=src,
            dst_ref=dst,
            send_sem=gsend.at[n],
            recv_sem=grecv.at[n],
            device_id=device,
            device_id_type=MESH,
        )

    erows = gcore.shape[2]
    last = experts - 1
    for at in range(n_m):
        gcore[at % 2, at // 2] = gacc[at % 2, at // 2].T[:erows]
    to_core = gate_copy(gcore.at[1 - core], gcore_in, 0, core_to)
    to_core.start()
    reduce_first(last)
    to_core.wait_recv()
    gcore[core] = gcore[core] + gcore_in[...]
    to_x = gate_copy(gcore.at[core, x_other], gx_in, 1, x_to)
    to_x.start()
    reduce_second(last - 1)
    reduce_third(last - 2)
    to_x.wait_recv()
    gt[t] = gcore[core, x_half] + gx_in[...]
    to_t = [gate_copy(gt.at[t], gt.at[t], 1 + j, (e, m, ahead(j))) for j in range(1, n_tp)]
    for copy in to_t:
        copy.start()
    reduce_second(last)
    reduce_third(last - 1)
    for j in range(1, n_tp):
        gate_copy(gt.at[behind(j)], gt.at[behind(j)], 1 + j, (e, m, ahead(j))).wait_recv()
    whole = gt[0]
    for j in range(1, n_tp):
        whole = whole + gt[j]
    gz[e] = whole
    to_z = [
        gate_copy(gz.at[e], gz.at[e], n_tp + k, (lax.rem(e + k, experts), m, t)) for k in range(1, experts)
    ]
    for copy in to_z:
        copy.start()
    for at in range(experts):
        rows = lax.broadcasted_iota(jnp.int32, (capacity, ntok), 0)
        place[at] = jnp.where(rows == slot_ref[at : at + 1, :], 1.0, 0.0).astype(BF16)
    reduce_third(last)
    for k in range(1, experts):
        src = gz.at[lax.rem(e + experts - k, experts)]
        gate_copy(src, src, n_tp + k, core_to).wait_recv()

    HIGHEST = lax.Precision.HIGHEST
    gates = []
    row = lax.broadcasted_iota(jnp.int32, gz.shape[1:], 0)
    for at in range(experts):
        line = jnp.sum(jnp.where(row == e, gz[at], 0.0), axis=0, keepdims=True)
        line = jnp.broadcast_to(line, (8, LANES))[:, :capacity]
        got = jnp.dot(line, place[at].astype(F32), precision=HIGHEST, preferred_element_type=F32)
        gates.append(got[0:1])
    picks = [[oh_ref[n, at : at + 1, :] for at in range(experts)] for n in range(TOP)]
    gate = [sum(picks[n][at] * gates[at] for at in range(experts)) for n in range(TOP)]
    first = first_ref[...]
    delta = first * (1.0 - first) * (gate[0] - gate[1])
    gate_ref[0:1] = gate[0]
    gate_ref[1:2] = gate[1]
    pad = -experts % 8
    zero = [jnp.zeros((pad, ntok), F32)] if pad else []
    dlog = jnp.concatenate([delta * (picks[0][at] - picks[1][at]) for at in range(experts)] + zero, axis=0)
    term = jnp.dot(dlog, tok_ref[...].astype(F32), precision=HIGHEST, preferred_element_type=F32)
    cols = width // n_ep
    for at in range(n_ep):
        terms[at, :, :cols] = term[:, at * cols : (at + 1) * cols]

    def term_copy(d):
        there = lax.rem(me + d, n_ep)
        return pltpu.make_async_remote_copy(
            src_ref=terms.at[there],
            dst_ref=terms_in.at[d],
            send_sem=tsend.at[d],
            recv_sem=trecv.at[d],
            device_id=ep_at(d),
            device_id_type=MESH,
        )

    def each(d, carry):
        term_copy(d).start()
        return carry

    lax.fori_loop(1, n_ep, each, 0)

    router_part = lax.dot_general(
        dlog, rw_ref[...], (((0,), (0,)), ((), ())), precision=HIGHEST, preferred_element_type=F32
    )
    spread = place[...].reshape(experts * capacity, ntok).T
    for k in range(1, experts):
        landed(home.at[lax.rem(e + k, experts)], RET, k)
    route_sum = jnp.dot(spread, home[...].reshape(experts * capacity, share), preferred_element_type=F32)
    grad_ref[...] = (route_sum + router_part).astype(BF16)

    def gather(d, total):
        term_copy(d).wait_recv()
        return total + terms_in[d, :, :cols]

    router_ref[...] = lax.fori_loop(1, n_ep, gather, terms[me, :, :cols])

    def done(d, carry):
        term_copy(d).wait_send()
        return carry

    lax.fori_loop(1, n_ep, done, 0)
    for copy in [to_core, to_x] + to_t + to_z:
        copy.wait_send()

    def finish(k, carry):
        mine = piece(k, m, t)
        @pl.when(k > 0)
        def _():
            sent(mine, Z, k)
            sent(mine_back(k), RET, k)
        sent(mine, X, k)
        sent(mine, CORE_OWN, k)
        sent(piece(k, x_peer, t), CORE_X, k)
        sent(core_in.at[k], R1, k)
        sent(across_a(k), R2A, k)
        sent(onward_b(k), R3B, k)
        for j in range(1, n_tp):
            sent(mine, y_kind(j), k)
            sent(piece(k, x_peer, t, last_cols), b_kind(j), k)
            sent(piece(k, m, behind(j), first_cols), a_kind(j), k)
            sent(piece(k, m, behind(j)), core_y(j), k)
            sent(piece(k, x_peer, behind(j), first_cols), core_a(j), k)
            sent(piece(k, x_peer, behind(j), last_cols), core_b(j), k)
            sent(across_b(k, j), r2b(j), k)
            sent(onward_a(k, j), r3a(j), k)
        pltpu.make_async_copy(full.at[k], x_hbm.at[k], out_sem.at[k]).wait()
        for copy in hidden_copies(k):
            copy.wait()
        return carry

    lax.fori_loop(0, experts, finish, 0)


def grads_kernel(x_ref, c_ref, dg_ref, du_ref, sc_ref, gg_ref, gu_ref, gd_ref, sct):
    @pl.when(pl.program_id(0) == 0)
    def _():
        sct[...] = sc_ref[...].T

    tile = x_ref.shape[-1]
    rows = dg_ref.shape[0]
    xt = x_ref[:, :, 0].reshape(rows, tile).T
    gg_ref[0] = jnp.dot(xt, dg_ref[...], preferred_element_type=F32)
    gu_ref[0] = jnp.dot(xt, du_ref[...], preferred_element_type=F32)
    gd_ref[0] = jnp.dot(sct[...], c_ref[:, :, 0].reshape(rows, tile), preferred_element_type=F32)


def shards(tokens, routes, router_weight, gate_proj, up_proj, down_proj, cotangent):
    ntok, width = tokens.shape
    experts = router_weight.shape[1]
    n_m, n_tp = lax.axis_size("m"), lax.axis_size("tp")
    share = width // n_tp
    capacity = min(ntok, 5 * TOP * ntok // (4 * experts))
    capacity = -(-capacity // 16) * 16
    tp_index = lax.axis_index("tp")
    ff = gate_proj.shape[2]

    logits = jnp.dot(tokens, router_weight, preferred_element_type=F32)
    onehot = (routes[:, :, None] == jnp.arange(experts, dtype=jnp.int32)[None, None, :]).astype(F32)
    chosen = jnp.sum(onehot * logits[:, None, :], axis=2)
    first = jax.nn.sigmoid(chosen[:, 0] - chosen[:, 1])
    gates = jnp.stack([first, 1.0 - first], axis=1)
    used = gates.astype(BF16)
    named = jnp.sum(onehot, axis=1)
    below = (jnp.arange(ntok)[:, None] > jnp.arange(ntok)[None, :]).astype(BF16)
    rank = jnp.dot(below, named.astype(BF16), preferred_element_type=F32)
    slot = jnp.where(named > 0, rank, -1.0).astype(jnp.int32)
    place = (
        jnp.arange(capacity, dtype=jnp.int32)[None, :, None] == slot.T[:, None, :]
    ).astype(BF16)
    gate_cols = jnp.sum(onehot * used.astype(F32)[:, :, None], axis=1).astype(BF16)
    payload = jnp.concatenate(
        [
            lax.dynamic_slice_in_dim(tokens, tp_index * share, share, 1),
            lax.dynamic_slice_in_dim(cotangent, tp_index * share, share, 1),
            gate_cols,
            jnp.zeros((ntok, LANES - experts), BF16),
        ],
        axis=1,
    )
    rows = jnp.dot(
        place.reshape(experts * capacity, ntok), payload, preferred_element_type=F32
    ).astype(BF16)
    wide = 2 * share + LANES
    rows = rows.reshape(experts, capacity, wide)

    held = n_m * capacity
    hid_shape = jax.ShapeDtypeStruct((experts, held, ff), BF16)
    flops = 2 * experts * held * width * ff
    kinds = 8 + 8 * (n_tp - 1)
    n_ep = experts * n_m
    half = share // 2
    erows = -(-experts // 8) * 8
    cols = width // n_ep
    router_rows = lax.dynamic_slice_in_dim(router_weight, tp_index * share, share, 0).astype(F32).T
    router_rows = jnp.pad(router_rows, ((0, erows - experts), (0, 0)))
    vmem = pl.BlockSpec(memory_space=pltpu.VMEM)
    anywhere = pl.BlockSpec(memory_space=pl.ANY)
    full_shape = (experts, n_m, n_tp, capacity, wide)
    full, d_gate, d_up, scaled, token_grad, gate_rows, router_rows_out = pl.pallas_call(
        functools.partial(rows_kernel, share),
        in_specs=[vmem] * 6 + [anywhere] * 3,
        out_specs=[anywhere] * 4 + [vmem] * 3,
        out_shape=[
            jax.ShapeDtypeStruct(full_shape, BF16),
            hid_shape,
            hid_shape,
            hid_shape,
            jax.ShapeDtypeStruct((ntok, share), BF16),
            jax.ShapeDtypeStruct((TOP, ntok), F32),
            jax.ShapeDtypeStruct((erows, cols), F32),
        ],
        scratch_shapes=[
            pltpu.VMEM(full_shape, BF16),
            pltpu.VMEM(gate_proj.shape, BF16),
            pltpu.VMEM(up_proj.shape, BF16),
            pltpu.VMEM(down_proj.shape, BF16),
            pltpu.VMEM(hid_shape.shape, BF16),
            pltpu.VMEM(hid_shape.shape, BF16),
            pltpu.VMEM(hid_shape.shape, BF16),
            pltpu.VMEM((experts, 2, 2, n_tp, capacity, share), BF16),
            pltpu.VMEM((experts, 2, n_tp, capacity, share), BF16),
            pltpu.VMEM((experts, n_tp, capacity, half), BF16),
            pltpu.VMEM((experts, n_tp - 1, 2, capacity, share - half), BF16),
            pltpu.VMEM((experts, n_tp - 1, capacity, half), BF16),
            pltpu.VMEM((experts, capacity, share - half), BF16),
            pltpu.VMEM((experts, capacity, share), BF16),
            pltpu.VMEM((experts, capacity, ntok), BF16),
            pltpu.VMEM((2, 2, LANES, LANES), F32),
            pltpu.VMEM((2, 2, erows, LANES), F32),
            pltpu.VMEM((2, erows, LANES), F32),
            pltpu.VMEM((erows, LANES), F32),
            pltpu.VMEM((n_tp, erows, LANES), F32),
            pltpu.VMEM((experts, erows, LANES), F32),
            pltpu.VMEM((n_ep, erows, LANES), F32),
            pltpu.VMEM((n_ep, erows, LANES), F32),
            pltpu.SemaphoreType.DMA((experts,)),
            pltpu.SemaphoreType.DMA((3, experts)),
            pltpu.SemaphoreType.DMA((kinds, experts)),
            pltpu.SemaphoreType.DMA((kinds, experts)),
            pltpu.SemaphoreType.DMA((4,)),
            pltpu.SemaphoreType.DMA((n_tp + experts,)),
            pltpu.SemaphoreType.DMA((n_tp + experts,)),
            pltpu.SemaphoreType.DMA((n_ep,)),
            pltpu.SemaphoreType.DMA((n_ep,)),
        ],
        compiler_params=pltpu.CompilerParams(
            collective_id=0, has_side_effects=True, vmem_limit_bytes=60 << 20
        ),
        cost_estimate=pl.CostEstimate(flops=5 * flops, bytes_accessed=30 << 20, transcendentals=0),
        name="rows",
    )(
        rows,
        tokens,
        slot.T,
        onehot.transpose(1, 2, 0),
        first[None, :],
        router_rows,
        gate_proj,
        up_proj,
        down_proj,
    )

    tile = 256
    per = share // tile
    total = experts * held
    whole = lambda i: (0, 0)
    grad_gate, grad_up, grad_down = pl.pallas_call(
        grads_kernel,
        grid=(width // tile,),
        in_specs=[
            pl.BlockSpec((experts, n_m, 1, capacity, tile), lambda i: (0, 0, i // per, 0, i % per)),
            pl.BlockSpec((experts, n_m, 1, capacity, tile), lambda i: (0, 0, i // per, 0, per + i % per)),
            pl.BlockSpec((total, ff), whole),
            pl.BlockSpec((total, ff), whole),
            pl.BlockSpec((total, ff), whole),
        ],
        out_specs=[
            pl.BlockSpec((1, tile, ff), lambda i: (0, i, 0)),
            pl.BlockSpec((1, tile, ff), lambda i: (0, i, 0)),
            pl.BlockSpec((1, ff, tile), lambda i: (0, 0, i)),
        ],
        out_shape=[
            jax.ShapeDtypeStruct(gate_proj.shape, F32),
            jax.ShapeDtypeStruct(up_proj.shape, F32),
            jax.ShapeDtypeStruct(down_proj.shape, F32),
        ],
        scratch_shapes=[pltpu.VMEM((ff, total), BF16)],
        cost_estimate=pl.CostEstimate(flops=3 * flops, bytes_accessed=30 << 20, transcendentals=0),
        name="grads",
    )(full, full, d_gate.reshape(total, ff), d_up.reshape(total, ff), scaled.reshape(total, ff))

    gate_grad = gate_rows.T
    router_grad = router_rows_out[:experts].T
    return (token_grad, gate_grad, router_grad, grad_gate, grad_up, grad_down)


def solution(mesh):
    devices = mesh.devices
    grid = Mesh(
        devices.reshape(devices.shape[0] // MEMBERS, MEMBERS, devices.shape[1]), ("e", "m", "tp")
    )
    ep = ("e", "m")
    return jax.shard_map(
        shards,
        mesh=grid,
        in_specs=(
            P(ep, None),
            P(ep, None),
            P(),
            P(ep, None, "tp"),
            P(ep, None, "tp"),
            P(ep, "tp", None),
            P(ep, None),
        ),
        out_specs=(
            P(ep, "tp"),
            P(ep, None),
            P(ep, None),
            P(ep, None, "tp"),
            P(ep, None, "tp"),
            P(ep, "tp", None),
        ),
        check_vma=False,
    )
```

```python
import functools

import jax
import jax.numpy as jnp
from jax import lax
from jax.experimental import pallas as pl
from jax.experimental.pallas import tpu as pltpu
from jax.sharding import Mesh, PartitionSpec as P

MEMBERS = 4
TOP = 2
LANES = 128
F32 = jnp.float32
BF16 = jnp.bfloat16
MESH = pl.DeviceIdType.MESH
NT = (((1,), (1,)), ((), ()))


def rows_kernel(
    share, tok_ref, cot_ref, route_ref, rw_ref, wg_hbm, wu_hbm, wd_hbm,
    gg_ref, gu_ref, gd_ref, grad_ref, gate_ref, router_ref,
    send_ref, full, wg_ref, wu_ref, wd_ref, dg_ref, du_ref, sc_ref, back, core_in, xa_in, yb_in, ya_in, xb_in, home, place,
    gacc, gcore, gcore_in, gx_in, gt, gz, terms, terms_in,
    send_sem, recv_sem, load_sem, gsend, grecv, tsend, trecv,
):
    experts, n_m, n_tp, capacity, _ = full.shape
    ntok, width = tok_ref.shape
    half = share // 2
    e, m, t = lax.axis_index("e"), lax.axis_index("m"), lax.axis_index("tp")
    n_ep = experts * n_m
    me = e * n_m + m
    x_half, core = lax.div(m, 2), lax.rem(m, 2)
    x_peer = lax.rem(m + 2, 4)
    core_peer = m + 1 - 2 * core
    held = n_m * capacity
    first_cols, last_cols = pl.ds(0, share), pl.ds(share, share + LANES)
    low, high = pl.ds(0, half), pl.ds(half, share - half)

    def ahead(j):
        return lax.rem(t + j, n_tp)

    def behind(j):
        return lax.rem(t + n_tp - j, n_tp)

    def ep_at(d):
        there = lax.rem(me + d, n_ep)
        return (lax.div(there, n_m), lax.rem(there, n_m), t)

    barrier = pltpu.get_barrier_semaphore()
    for d in range(1, n_ep):
        pl.semaphore_signal(barrier, inc=1, device_id=ep_at(d), device_id_type=MESH)
    for j in range(1, n_tp):
        pl.semaphore_signal(barrier, inc=1, device_id=(e, m, ahead(j)), device_id_type=MESH)
    loads = [
        pltpu.make_async_copy(src, dst, load_sem.at[n])
        for n, (src, dst) in enumerate([(wg_hbm, wg_ref), (wu_hbm, wu_ref), (wd_hbm, wd_ref)])
    ]
    for load in loads:
        load.start()

    logits = lax.dot_general(rw_ref[...], tok_ref[...], NT, preferred_element_type=F32)
    picks = [
        [jnp.where(route_ref[n : n + 1, :] == at, 1.0, 0.0) for at in range(experts)] for n in range(TOP)
    ]
    chosen = [sum(picks[n][at] * logits[at : at + 1] for at in range(experts)) for n in range(TOP)]
    first = jax.nn.sigmoid(chosen[0] - chosen[1])
    used = [gate.astype(BF16).astype(F32) for gate in (first, 1.0 - first)]
    pad = -experts % 8
    blank = [jnp.zeros((pad, ntok), F32)] if pad else []
    named = jnp.concatenate([picks[0][at] + picks[1][at] for at in range(experts)] + blank, axis=0)
    order = lax.broadcasted_iota(jnp.int32, (ntok, ntok), 0) < lax.broadcasted_iota(jnp.int32, (ntok, ntok), 1)
    rank = jnp.dot(named.astype(BF16), jnp.where(order, 1.0, 0.0).astype(BF16), preferred_element_type=F32)
    slot = jnp.where(named > 0.0, rank, -1.0).astype(jnp.int32)
    line = lax.broadcasted_iota(jnp.int32, (capacity, ntok), 0)
    for at in range(experts):
        chosen_slot = jnp.where(line == slot[at : at + 1], 1.0, 0.0)
        place[at] = chosen_slot.astype(BF16)
        gate_row = picks[0][at] * used[0] + picks[1][at] * used[1]
        gate_col = jnp.sum(chosen_slot * gate_row, axis=1, keepdims=True)
        send_ref[at, :, 2 * share :] = jnp.broadcast_to(gate_col, (capacity, LANES)).astype(BF16)
    mine_cols = pl.ds(pl.multiple_of(t * share, LANES), share)
    spots = place[...].reshape(experts * capacity, ntok)
    for n, ref in enumerate((tok_ref, cot_ref)):
        rows = jnp.dot(spots, ref[:, mine_cols], preferred_element_type=F32).astype(BF16)
        send_ref[:, :, n * share : (n + 1) * share] = rows.reshape(experts, capacity, share)
    keep = pltpu.make_async_copy(send_ref.at[e], full.at[e, m, t], load_sem.at[3])
    keep.start()
    for ref in (gacc, gg_ref, gu_ref, gd_ref):
        ref[...] = jnp.zeros_like(ref)
    pl.semaphore_wait(barrier, n_ep - 1 + n_tp - 1)

    near = lax.min(e, experts - 1 - e)
    side = 1 - 2 * lax.div(2 * e, experts)

    def source(i):
        step, both = lax.div(i + 1, 2), i <= 2 * near
        away = jnp.where(both, step, i - near)
        return e + side * jnp.where(both & (lax.rem(i, 2) == 0), -away, away)

    def remote(src, dst, kind, k, device):
        return pltpu.make_async_remote_copy(
            src_ref=src,
            dst_ref=dst,
            send_sem=send_sem.at[kind, k],
            recv_sem=recv_sem.at[kind, k],
            device_id=device,
            device_id_type=MESH,
        )

    def piece(k, src_m, src_t, cols=None):
        ref = full.at[k, src_m, src_t]
        return ref if cols is None else ref.at[:, cols]

    others = n_tp - 1
    X, CORE_OWN, CORE_X, Z, R1, R2A, R3B, RET = range(8)
    def y_kind(j): return 8 + (j - 1)
    def a_kind(j): return 8 + others + (j - 1)
    def b_kind(j): return 8 + 2 * others + (j - 1)
    def core_y(j): return 8 + 3 * others + (j - 1)
    def core_a(j): return 8 + 4 * others + (j - 1)
    def core_b(j): return 8 + 5 * others + (j - 1)
    def r2b(j): return 8 + 6 * others + (j - 1)
    def r3a(j): return 8 + 7 * others + (j - 1)

    x_to, core_to = (e, x_peer, t), (e, core_peer, t)

    def pass_on(ref, kind, k, device):
        remote(ref, ref, kind, k, device).start()

    def landed(ref, kind, k):
        remote(ref, ref, kind, k, core_to).wait_recv()

    def sent(ref, kind, k):
        remote(ref, ref, kind, k, core_to).wait_send()

    def own(k, away):
        mine = piece(k, m, t)

        @pl.when(away)
        def _():
            landed(mine, Z, k)
            pass_on(mine, X, k, x_to)
            for j in range(1, n_tp):
                pass_on(mine, y_kind(j), k, (e, m, ahead(j)))
            pass_on(mine, CORE_OWN, k, core_to)

        @pl.when(jnp.logical_not(away))
        def _():
            src = send_ref.at[e]
            remote(src, mine, X, k, x_to).start()
            for j in range(1, n_tp):
                remote(src, mine, y_kind(j), k, (e, m, ahead(j))).start()
            remote(src, mine, CORE_OWN, k, core_to).start()

    def neighbours(k):
        across = piece(k, x_peer, t)
        landed(across, X, k)
        for j in range(1, n_tp):
            pass_on(piece(k, x_peer, t, last_cols), b_kind(j), k, (e, m, ahead(j)))
        pass_on(across, CORE_X, k, core_to)
        for j in range(1, n_tp):
            beside = piece(k, m, behind(j))
            landed(beside, y_kind(j), k)
            pass_on(piece(k, m, behind(j), first_cols), a_kind(j), k, x_to)
            pass_on(beside, core_y(j), k, core_to)

    def corners(k):
        for j in range(1, n_tp):
            for cols, kind, across in ((first_cols, a_kind, core_a), (last_cols, b_kind, core_b)):
                ref = piece(k, x_peer, behind(j), cols)
                landed(ref, kind(j), k)
                pass_on(ref, across(j), k, core_to)

    other_x = lax.rem(core_peer + 2, 4)

    def partner(k):
        landed(piece(k, core_peer, t), CORE_OWN, k)
        landed(piece(k, other_x, t), CORE_X, k)
        for j in range(1, n_tp):
            landed(piece(k, core_peer, behind(j)), core_y(j), k)
            landed(piece(k, other_x, behind(j), first_cols), core_a(j), k)
            landed(piece(k, other_x, behind(j), last_cols), core_b(j), k)

    def compute(n):
        k = source(n)

        def part(tp_at, base, size):
            return full[k, :, tp_at, :, base : base + size].reshape(held, size)

        def contract(base, w_ref, nt):
            total = None
            for tp_at in range(n_tp):
                cols = slice(tp_at * share, (tp_at + 1) * share)
                rows = part(tp_at, base, share)
                if nt:
                    term = lax.dot_general(rows, w_ref[0, :, cols], NT, preferred_element_type=F32)
                else:
                    term = jnp.dot(rows, w_ref[0, cols, :], preferred_element_type=F32)
                total = term if total is None else total + term
            return total

        gpre = contract(0, wg_ref, False)
        upre = contract(0, wu_ref, False)
        qvals = contract(share, wd_ref, True)
        extra = part(0, 2 * share, LANES).astype(F32)
        lane = lax.broadcasted_iota(jnp.int32, extra.shape, 1)
        weight = extra[:, :1]
        sig = jax.nn.sigmoid(gpre)
        silu_val = gpre * sig
        hidden = (silu_val * upre).astype(BF16).astype(F32)
        gate_part = jnp.sum(hidden * qvals, axis=1, keepdims=True)
        dhid = weight * qvals
        d_gate = (dhid * upre * sig * (1.0 + gpre * (1.0 - sig))).astype(BF16)
        d_up = (dhid * silu_val).astype(BF16)
        dg_ref[n] = d_gate
        du_ref[n] = d_up
        sc_ref[n] = (weight * hidden).astype(BF16)
        gate_lanes = jnp.where(lane == k, gate_part, 0.0).reshape(n_m, capacity, LANES)
        for at in range(n_m):
            gacc[at % 2, at // 2, :capacity, :] += gate_lanes[at]
        for tp_at in range(n_tp):
            cols = slice(tp_at * share, (tp_at + 1) * share)
            grad = lax.dot_general(d_gate, wg_ref[0, cols, :], NT, preferred_element_type=F32)
            grad = grad + lax.dot_general(d_up, wu_ref[0, cols, :], NT, preferred_element_type=F32)
            grad = grad.astype(BF16).reshape(n_m, capacity, share)
            for at in range(n_m):
                back[k, at % 2, at // 2, tp_at] = grad[at]
        remote(back.at[k, 1 - core], core_in.at[k], R1, k, core_to).start()

    group = 2 - experts % 2

    def weight_grads(n, part):
        tp_at, down = part // 2, part % 2
        cols = slice(tp_at * share, (tp_at + 1) * share)

        def rows(base):
            parts = [full[source(n + g), :, tp_at, :, base : base + share] for g in range(group)]
            return jnp.concatenate([at.reshape(held, share) for at in parts], axis=0)

        def units(ref):
            return ref[pl.ds(n, group)].reshape(group * held, -1)

        if down:
            gd_ref[0, :, cols] += jnp.dot(units(sc_ref).T, rows(share), preferred_element_type=F32)
        else:
            flipped = rows(0).T
            gg_ref[0, cols, :] += jnp.dot(flipped, units(dg_ref), preferred_element_type=F32)
            gu_ref[0, cols, :] += jnp.dot(flipped, units(du_ref), preferred_element_type=F32)

    def add(*terms):
        total = terms[0].astype(F32)
        for term in terms[1:]:
            total = total + term.astype(F32)
        return total.astype(BF16)

    x_other = 1 - x_half

    def across_a(k):
        return back.at[k, core, x_other, :, :, low]

    def across_b(k, j):
        return back.at[k, core, :, ahead(j), :, high]

    def reduce_first(k):
        landed(core_in.at[k], R1, k)
        back[k, core] = add(back[k, core], core_in[k])
        remote(across_a(k), xa_in.at[k], R2A, k, x_to).start()
        for j in range(1, n_tp):
            remote(across_b(k, j), yb_in.at[k, j - 1], r2b(j), k, (e, m, ahead(j))).start()

    def onward_a(k, j):
        return back.at[k, core, x_half, ahead(j), :, low]

    def onward_b(k):
        return back.at[k, core, x_other, t, :, high]

    def reduce_second(k):
        landed(xa_in.at[k], R2A, k)
        for j in range(1, n_tp):
            onward_a(k, j)[...] = add(onward_a(k, j)[...], xa_in[k, ahead(j)])
            remote(onward_a(k, j), ya_in.at[k, j - 1], r3a(j), k, (e, m, ahead(j))).start()
        for j in range(1, n_tp):
            landed(yb_in.at[k, j - 1], r2b(j), k)
        onward_b(k)[...] = add(onward_b(k)[...], *[yb_in[k, j - 1, x_other] for j in range(1, n_tp)])
        remote(onward_b(k), xb_in.at[k], R3B, k, x_to).start()

    def mine_back(k):
        return back.at[k, core, x_half, t]

    def reduce_third(k):
        for j in range(1, n_tp):
            landed(ya_in.at[k, j - 1], r3a(j), k)
        landed(xb_in.at[k], R3B, k)
        ref = mine_back(k)
        ref[:, :half] = add(ref[:, :half], xa_in[k, t], *[ya_in[k, j - 1] for j in range(1, n_tp)])
        ref[:, half:] = add(ref[:, half:], xb_in[k], *[yb_in[k, j - 1, x_half] for j in range(1, n_tp)])

        @pl.when(k != e)
        def _():
            ret_copy(k, e).start()

        @pl.when(k == e)
        def _():
            home[e] = ref[...]

    def ret_copy(k, at):
        return pltpu.make_async_remote_copy(
            src_ref=mine_back(k),
            dst_ref=home.at[at],
            send_sem=send_sem.at[RET, k],
            recv_sem=recv_sem.at[RET, at],
            device_id=(k, m, t),
            device_id_type=MESH,
        )

    def send_z(i, carry):
        there = source(i)
        z_copy(there, e).start()
        return carry

    def z_copy(there, at):
        return pltpu.make_async_remote_copy(
            src_ref=send_ref.at[there],
            dst_ref=full.at[at, m, t],
            send_sem=send_sem.at[Z, there],
            recv_sem=recv_sem.at[Z, at],
            device_id=(there, m, t),
            device_id_type=MESH,
        )

    lax.fori_loop(1, experts, send_z, 0)

    def step(i, carry):
        pl.when((i >= 1) & (i < experts + 1))(lambda: neighbours(source(i - 1)))
        pl.when(i >= 2)(lambda: corners(source(i - 2)))
        pl.when(i < experts)(lambda: own(source(i), i > 0))
        pl.when(i >= 3)(lambda: reduce_first(source(i - 3)))
        pl.when(i >= 4)(lambda: reduce_second(source(i - 4)))
        pl.when(i >= 5)(lambda: reduce_third(source(i - 5)))

        @pl.when(i == 2)
        def _():
            keep.wait()
            for load in loads:
                load.wait()

        @pl.when(i >= 2)
        def _():
            partner(source(i - 2))
            compute(i - 2)

        @pl.when((i >= 1 + group) & (lax.rem(i - 1, group) == 0) & (i < experts + 1))
        def _():
            for part in range(2 * n_tp):
                weight_grads(i - 1 - group, part)

        return carry

    lax.fori_loop(0, experts + 2, step, 0)

    def gate_copy(src, dst, n, device):
        return pltpu.make_async_remote_copy(
            src_ref=src,
            dst_ref=dst,
            send_sem=gsend.at[n],
            recv_sem=grecv.at[n],
            device_id=device,
            device_id_type=MESH,
        )

    erows = gcore.shape[2]
    last, second, third = [source(experts - n) for n in (1, 2, 3)]
    for at in range(n_m):
        gcore[at % 2, at // 2] = gacc[at % 2, at // 2].T[:erows]
    to_core = gate_copy(gcore.at[1 - core], gcore_in, 0, core_to)
    to_core.start()
    reduce_first(last)
    rest = [functools.partial(weight_grads, experts - group, part) for part in range(2 * n_tp)]
    rest.pop()()
    to_core.wait_recv()
    gcore[core] = gcore[core] + gcore_in[...]
    to_x = gate_copy(gcore.at[core, x_other], gx_in, 1, x_to)
    to_x.start()
    reduce_second(second)
    reduce_third(third)
    rest.pop()()
    to_x.wait_recv()
    gt[t] = gcore[core, x_half] + gx_in[...]
    to_t = [gate_copy(gt.at[t], gt.at[t], 1 + j, (e, m, ahead(j))) for j in range(1, n_tp)]
    for copy in to_t:
        copy.start()
    reduce_second(last)
    reduce_third(second)
    for part in rest:
        part()
    for j in range(1, n_tp):
        gate_copy(gt.at[behind(j)], gt.at[behind(j)], 1 + j, (e, m, ahead(j))).wait_recv()
    whole = gt[0]
    for j in range(1, n_tp):
        whole = whole + gt[j]
    gz[e] = whole
    to_z = [
        gate_copy(gz.at[e], gz.at[e], n_tp + k, (lax.rem(e + k, experts), m, t)) for k in range(1, experts)
    ]
    for copy in to_z:
        copy.start()
    for k in range(1, experts):
        src = gz.at[lax.rem(e + experts - k, experts)]
        gate_copy(src, src, n_tp + k, core_to).wait_recv()

    HIGHEST = lax.Precision.HIGHEST
    gates = []
    row = lax.broadcasted_iota(jnp.int32, gz.shape[1:], 0)
    for at in range(experts):
        line = jnp.sum(jnp.where(row == e, gz[at], 0.0), axis=0, keepdims=True)
        line = jnp.broadcast_to(line, (8, LANES))[:, :capacity]
        got = jnp.dot(line, place[at].astype(F32), precision=HIGHEST, preferred_element_type=F32)
        gates.append(got[0:1])
    gate = [sum(picks[n][at] * gates[at] for at in range(experts)) for n in range(TOP)]
    delta = first * (1.0 - first) * (gate[0] - gate[1])
    gate_ref[0:1] = gate[0]
    gate_ref[1:2] = gate[1]
    dlog = jnp.concatenate([delta * (picks[0][at] - picks[1][at]) for at in range(experts)] + blank, axis=0)
    term = jnp.dot(dlog, tok_ref[...].astype(F32), precision=HIGHEST, preferred_element_type=F32)
    cols = width // n_ep
    for at in range(n_ep):
        terms[at, :, :cols] = term[:, at * cols : (at + 1) * cols]

    def term_copy(d):
        there = lax.rem(me + d, n_ep)
        return pltpu.make_async_remote_copy(
            src_ref=terms.at[there],
            dst_ref=terms_in.at[d],
            send_sem=tsend.at[d],
            recv_sem=trecv.at[d],
            device_id=ep_at(d),
            device_id_type=MESH,
        )

    def each(d, carry):
        term_copy(d).start()
        return carry

    lax.fori_loop(1, n_ep, each, 0)

    reduce_third(last)
    weight_rows = [rw_ref[:, mine_cols].astype(F32)] + ([jnp.zeros((pad, share), F32)] if pad else [])
    router_part = lax.dot_general(
        dlog, jnp.concatenate(weight_rows, axis=0), (((0,), (0,)), ((), ())), precision=HIGHEST, preferred_element_type=F32
    )
    spread = place[...].reshape(experts * capacity, ntok).T
    for k in range(1, experts):
        at = lax.rem(e + k, experts)
        ret_copy(at, at).wait_recv()
    route_sum = jnp.dot(spread, home[...].reshape(experts * capacity, share), preferred_element_type=F32)
    grad_ref[...] = (route_sum + router_part).astype(BF16)

    def gather(d, total):
        term_copy(d).wait_recv()
        return total + terms_in[d, :, :cols]

    router_ref[...] = lax.fori_loop(1, n_ep, gather, terms[me, :, :cols])[:experts]

    def done(d, carry):
        term_copy(d).wait_send()
        return carry

    lax.fori_loop(1, n_ep, done, 0)
    for copy in [to_core, to_x] + to_t + to_z:
        copy.wait_send()

    def finish(k, carry):
        mine = piece(k, m, t)

        @pl.when(k != e)
        def _():
            sent(mine, Z, k)
            sent(mine_back(k), RET, k)

        sent(mine, X, k)
        sent(mine, CORE_OWN, k)
        sent(piece(k, x_peer, t), CORE_X, k)
        sent(core_in.at[k], R1, k)
        sent(across_a(k), R2A, k)
        sent(onward_b(k), R3B, k)
        for j in range(1, n_tp):
            sent(mine, y_kind(j), k)
            sent(piece(k, x_peer, t, last_cols), b_kind(j), k)
            sent(piece(k, m, behind(j), first_cols), a_kind(j), k)
            sent(piece(k, m, behind(j)), core_y(j), k)
            sent(piece(k, x_peer, behind(j), first_cols), core_a(j), k)
            sent(piece(k, x_peer, behind(j), last_cols), core_b(j), k)
            sent(across_b(k, j), r2b(j), k)
            sent(onward_a(k, j), r3a(j), k)
        return carry

    lax.fori_loop(0, experts, finish, 0)


def hand_over(*refs):
    n = len(refs) // 2
    copies = [
        pltpu.make_async_copy(src, dst, refs[-1].at[at])
        for at, (src, dst) in enumerate(zip(refs[:n], refs[n:-1]))
    ]
    for copy in copies:
        copy.start()
    for copy in copies:
        copy.wait()


def shards(tokens, routes, router_weight, gate_proj, up_proj, down_proj, cotangent):
    ntok, width = tokens.shape
    experts = router_weight.shape[1]
    n_m, n_tp = lax.axis_size("m"), lax.axis_size("tp")
    share = width // n_tp
    capacity = min(ntok, 5 * TOP * ntok // (4 * experts))
    capacity = -(-capacity // 16) * 16
    ff = gate_proj.shape[2]

    wide = 2 * share + LANES
    held = n_m * capacity
    hid_shape = jax.ShapeDtypeStruct((experts, held, ff), BF16)
    flops = 2 * experts * held * width * ff
    kinds = 8 + 8 * (n_tp - 1)
    n_ep = experts * n_m
    half = share // 2
    erows = -(-experts // 8) * 8
    cols = width // n_ep
    vmem = pl.BlockSpec(memory_space=pltpu.VMEM)
    anywhere = pl.BlockSpec(memory_space=pl.ANY)
    full_shape = (experts, n_m, n_tp, capacity, wide)
    grad_gate, grad_up, grad_down, token_grad, gate_rows, router_rows = pl.pallas_call(
        functools.partial(rows_kernel, share),
        in_specs=[vmem] * 4 + [anywhere] * 3,
        out_specs=[vmem] * 6,
        out_shape=[
            pltpu.VMEM(gate_proj.shape, F32),
            pltpu.VMEM(up_proj.shape, F32),
            pltpu.VMEM(down_proj.shape, F32),
            pltpu.VMEM((ntok, share), BF16),
            pltpu.VMEM((TOP, ntok), F32),
            pltpu.VMEM((experts, cols), F32),
        ],
        scratch_shapes=[
            pltpu.VMEM((experts, capacity, wide), BF16),
            pltpu.VMEM(full_shape, BF16),
            pltpu.VMEM(gate_proj.shape, BF16),
            pltpu.VMEM(up_proj.shape, BF16),
            pltpu.VMEM(down_proj.shape, BF16),
            pltpu.VMEM(hid_shape.shape, BF16),
            pltpu.VMEM(hid_shape.shape, BF16),
            pltpu.VMEM(hid_shape.shape, BF16),
            pltpu.VMEM((experts, 2, 2, n_tp, capacity, share), BF16),
            pltpu.VMEM((experts, 2, n_tp, capacity, share), BF16),
            pltpu.VMEM((experts, n_tp, capacity, half), BF16),
            pltpu.VMEM((experts, n_tp - 1, 2, capacity, share - half), BF16),
            pltpu.VMEM((experts, n_tp - 1, capacity, half), BF16),
            pltpu.VMEM((experts, capacity, share - half), BF16),
            pltpu.VMEM((experts, capacity, share), BF16),
            pltpu.VMEM((experts, capacity, ntok), BF16),
            pltpu.VMEM((2, 2, LANES, LANES), F32),
            pltpu.VMEM((2, 2, erows, LANES), F32),
            pltpu.VMEM((2, erows, LANES), F32),
            pltpu.VMEM((erows, LANES), F32),
            pltpu.VMEM((n_tp, erows, LANES), F32),
            pltpu.VMEM((experts, erows, LANES), F32),
            pltpu.VMEM((n_ep, erows, LANES), F32),
            pltpu.VMEM((n_ep, erows, LANES), F32),
            pltpu.SemaphoreType.DMA((kinds, experts)),
            pltpu.SemaphoreType.DMA((kinds, experts)),
            pltpu.SemaphoreType.DMA((4,)),
            pltpu.SemaphoreType.DMA((n_tp + experts,)),
            pltpu.SemaphoreType.DMA((n_tp + experts,)),
            pltpu.SemaphoreType.DMA((n_ep,)),
            pltpu.SemaphoreType.DMA((n_ep,)),
        ],
        compiler_params=pltpu.CompilerParams(
            collective_id=0, has_side_effects=True, vmem_limit_bytes=46 << 20
        ),
        cost_estimate=pl.CostEstimate(flops=5 * flops, bytes_accessed=30 << 20, transcendentals=0),
        name="rows",
    )(
        tokens,
        cotangent,
        routes.T,
        router_weight.T,
        gate_proj,
        up_proj,
        down_proj,
    )

    results = (grad_gate, grad_up, grad_down, token_grad, gate_rows, router_rows)
    grad_gate, grad_up, grad_down, token_grad, gate_rows, router_rows = pl.pallas_call(
        hand_over,
        in_specs=[vmem] * 6,
        out_specs=[anywhere] * 6,
        out_shape=[jax.ShapeDtypeStruct(at.shape, at.dtype) for at in results],
        scratch_shapes=[pltpu.SemaphoreType.DMA((6,))],
        compiler_params=pltpu.CompilerParams(vmem_limit_bytes=1 << 20),
        name="hand_over",
    )(*results)
    return (token_grad, gate_rows.T, router_rows.T, grad_gate, grad_up, grad_down)


def solution(mesh):
    devices = mesh.devices
    grid = Mesh(
        devices.reshape(devices.shape[0] // MEMBERS, MEMBERS, devices.shape[1]), ("e", "m", "tp")
    )
    ep = ("e", "m")
    return jax.shard_map(
        shards,
        mesh=grid,
        in_specs=(
            P(ep, None),
            P(ep, None),
            P(),
            P(ep, None, "tp"),
            P(ep, None, "tp"),
            P(ep, "tp", None),
            P(ep, None),
        ),
        out_specs=(
            P(ep, "tp"),
            P(ep, None),
            P(ep, None),
            P(ep, None, "tp"),
            P(ep, None, "tp"),
            P(ep, "tp", None),
        ),
        check_vma=False,
    )
```

```python
import functools

import jax
import jax.numpy as jnp
from jax import lax
from jax.experimental import pallas as pl
from jax.experimental.pallas import tpu as pltpu
from jax.sharding import Mesh, PartitionSpec as P

MEMBERS = 4
TOP = 2
LANES = 128
F32 = jnp.float32
BF16 = jnp.bfloat16
MESH = pl.DeviceIdType.MESH
NT = (((1,), (1,)), ((), ()))


def rows_kernel(
    share, tok_ref, cot_ref, route_ref, rw_ref, wg_hbm, wu_hbm, wd_hbm,
    gg_ref, gu_ref, gd_ref, grad_ref, gate_ref, router_ref,
    send_ref, gw, gw_in, full, wg_ref, wu_ref, wd_ref, dg_ref, du_ref, sc_ref, back, core_in, xa_in, yb_in, ya_in, xb_in, home, place,
    gacc, gcore, gcore_in, gx_in, gt, gz, terms, terms_in,
    send_sem, recv_sem, load_sem, gsend, grecv, tsend, trecv, wsend, wrecv,
):
    experts, n_m, n_tp, capacity, _ = full.shape
    ntok, width = tok_ref.shape
    half = share // 2
    e, m, t = lax.axis_index("e"), lax.axis_index("m"), lax.axis_index("tp")
    n_ep = experts * n_m
    me = e * n_m + m
    x_half, core = lax.div(m, 2), lax.rem(m, 2)
    x_peer = lax.rem(m + 2, 4)
    core_peer = m + 1 - 2 * core
    held = n_m * capacity
    first_cols, last_cols = pl.ds(0, share), pl.ds(share, share)
    low, high = pl.ds(0, half), pl.ds(half, share - half)

    def ahead(j):
        return lax.rem(t + j, n_tp)

    def behind(j):
        return lax.rem(t + n_tp - j, n_tp)

    def ep_at(d):
        there = lax.rem(me + d, n_ep)
        return (lax.div(there, n_m), lax.rem(there, n_m), t)

    barrier = pltpu.get_barrier_semaphore()
    for d in range(1, n_ep):
        pl.semaphore_signal(barrier, inc=1, device_id=ep_at(d), device_id_type=MESH)
    for j in range(1, n_tp):
        pl.semaphore_signal(barrier, inc=1, device_id=(e, m, ahead(j)), device_id_type=MESH)
    loads = [
        pltpu.make_async_copy(src, dst, load_sem.at[n])
        for n, (src, dst) in enumerate([(wg_hbm, wg_ref), (wu_hbm, wu_ref), (wd_hbm, wd_ref)])
    ]
    for load in loads:
        load.start()

    logits = lax.dot_general(rw_ref[...], tok_ref[...], NT, preferred_element_type=F32)
    picks = [
        [jnp.where(route_ref[n : n + 1, :] == at, 1.0, 0.0) for at in range(experts)] for n in range(TOP)
    ]
    chosen = [sum(picks[n][at] * logits[at : at + 1] for at in range(experts)) for n in range(TOP)]
    first = jax.nn.sigmoid(chosen[0] - chosen[1])
    used = [gate.astype(BF16).astype(F32) for gate in (first, 1.0 - first)]
    pad = -experts % 8
    blank = [jnp.zeros((pad, ntok), F32)] if pad else []
    named = jnp.concatenate([picks[0][at] + picks[1][at] for at in range(experts)] + blank, axis=0)
    order = lax.broadcasted_iota(jnp.int32, (ntok, ntok), 0) < lax.broadcasted_iota(jnp.int32, (ntok, ntok), 1)
    rank = jnp.dot(named.astype(BF16), jnp.where(order, 1.0, 0.0).astype(BF16), preferred_element_type=F32)
    slot = jnp.where(named > 0.0, rank, -1.0).astype(jnp.int32)
    line = lax.broadcasted_iota(jnp.int32, (capacity, ntok), 0)
    for at in range(experts):
        chosen_slot = jnp.where(line == slot[at : at + 1], 1.0, 0.0)
        place[at] = chosen_slot.astype(BF16)
        gate_row = (picks[0][at] * used[0] + picks[1][at] * used[1]).astype(BF16)
        gw[at, :, :capacity] = lax.dot_general(
            jnp.broadcast_to(gate_row, (8, ntok)), place[at], NT, preferred_element_type=F32
        )
    gw_in[me] = gw[e]
    mine_cols = pl.ds(pl.multiple_of(t * share, LANES), share)
    spots = place[...].reshape(experts * capacity, ntok)
    for n, ref in enumerate((tok_ref, cot_ref)):
        rows = jnp.dot(spots, ref[:, mine_cols], preferred_element_type=F32).astype(BF16)
        send_ref[:, :, n * share : (n + 1) * share] = rows.reshape(experts, capacity, share)
    for tp_at in range(n_tp):
        cols = slice(tp_at * share, (tp_at + 1) * share)
        for n, ref in enumerate((tok_ref, cot_ref)):
            rows = jnp.dot(place[e], ref[:, cols], preferred_element_type=F32)
            full[e, m, tp_at, :, n * share : (n + 1) * share] = rows.astype(BF16)
    gacc[...] = jnp.zeros_like(gacc)
    pl.semaphore_wait(barrier, n_ep - 1 + n_tp - 1)

    near = lax.min(e, experts - 1 - e)
    side = 1 - 2 * lax.div(2 * e, experts)

    def source(i):
        step, both = lax.div(i + 1, 2), i <= 2 * near
        away = jnp.where(both, step, i - near)
        return e + side * jnp.where(both & (lax.rem(i, 2) == 0), -away, away)

    def remote(src, dst, kind, k, device):
        return pltpu.make_async_remote_copy(
            src_ref=src,
            dst_ref=dst,
            send_sem=send_sem.at[kind, k],
            recv_sem=recv_sem.at[kind, k],
            device_id=device,
            device_id_type=MESH,
        )

    def piece(k, src_m, src_t, cols=None):
        ref = full.at[k, src_m, src_t]
        return ref if cols is None else ref.at[:, cols]

    others = n_tp - 1
    X, CORE_OWN, CORE_X, Z, R1, R2A, R3B, RET = 0, 2, 4, 6, 8, 9, 10, 11
    def y_kind(j): return 12 + 2 * (j - 1)
    def core_y(j): return 12 + 2 * others + 2 * (j - 1)
    def a_kind(j): return 12 + 4 * others + (j - 1)
    def b_kind(j): return 12 + 5 * others + (j - 1)
    def core_a(j): return 12 + 6 * others + (j - 1)
    def core_b(j): return 12 + 7 * others + (j - 1)
    def r2b(j): return 12 + 8 * others + (j - 1)
    def r3a(j): return 12 + 9 * others + (j - 1)

    parts = (first_cols, last_cols)

    x_to, core_to = (e, x_peer, t), (e, core_peer, t)

    def pass_on(ref, kind, k, device):
        remote(ref, ref, kind, k, device).start()

    def landed(ref, kind, k):
        remote(ref, ref, kind, k, core_to).wait_recv()

    def sent(ref, kind, k):
        remote(ref, ref, kind, k, core_to).wait_send()

    def own(k, h):
        mine = piece(k, m, t, parts[h])
        landed(mine, Z + h, k)
        pass_on(mine, X + h, k, x_to)
        for j in range(1, n_tp):
            pass_on(mine, y_kind(j) + h, k, (e, m, ahead(j)))
        pass_on(mine, CORE_OWN + h, k, core_to)

    def neighbours(k, h):
        across = piece(k, x_peer, t, parts[h])

        def along_y():
            for j in range(1, n_tp):
                beside = piece(k, m, behind(j), parts[h])
                landed(beside, y_kind(j) + h, k)
                if h == 0:
                    pass_on(beside, a_kind(j), k, x_to)
                pass_on(beside, core_y(j) + h, k, core_to)

        if h == 0:
            along_y()
        landed(across, X + h, k)
        if h == 1:
            for j in range(1, n_tp):
                pass_on(across, b_kind(j), k, (e, m, ahead(j)))
        pass_on(across, CORE_X + h, k, core_to)
        if h == 1:
            along_y()

    def corners(k):
        for j in range(1, n_tp):
            for cols, kind, across in ((first_cols, a_kind, core_a), (last_cols, b_kind, core_b)):
                ref = piece(k, x_peer, behind(j), cols)
                landed(ref, kind(j), k)
                pass_on(ref, across(j), k, core_to)

    def own_here():
        pass_on(piece(e, m, t), X, e, x_to)
        for j in range(1, n_tp):
            pass_on(piece(e, m, ahead(j), first_cols), a_kind(j), e, x_to)
        pass_on(full.at[e, m], CORE_OWN, e, core_to)

    def neighbours_here():
        across = piece(e, x_peer, t)
        landed(across, X, e)
        for j in range(1, n_tp):
            pass_on(piece(e, x_peer, t, last_cols), b_kind(j), e, (e, m, ahead(j)))
        pass_on(across, CORE_X, e, core_to)

    def corners_here():
        for j in range(1, n_tp):
            ref = piece(e, x_peer, ahead(j), first_cols)
            landed(ref, a_kind(j), e)
            pass_on(ref, core_a(j), e, core_to)
            ref = piece(e, x_peer, behind(j), last_cols)
            landed(ref, b_kind(j), e)
            pass_on(ref, core_b(j), e, core_to)

    other_x = lax.rem(core_peer + 2, 4)

    def partner_here():
        landed(full.at[e, core_peer], CORE_OWN, e)
        landed(piece(e, other_x, t), CORE_X, e)
        for j in range(1, n_tp):
            landed(piece(e, other_x, ahead(j), first_cols), core_a(j), e)
            landed(piece(e, other_x, behind(j), last_cols), core_b(j), e)

    def weight_copy(d):
        there = ep_at(d)
        return pltpu.make_async_remote_copy(
            src_ref=gw.at[there[0]],
            dst_ref=gw_in.at[me],
            send_sem=wsend.at[d],
            recv_sem=wrecv.at[d],
            device_id=there,
            device_id_type=MESH,
        )

    def weights(k):
        for at in range(n_m):
            d = lax.rem(me + n_ep - k * n_m - at, n_ep)
            pl.when(d > 0)(lambda d=d: weight_copy(d).wait_recv())
        lines = gw_in[pl.ds(k * n_m, n_m)].reshape(n_m * 8, LANES).T
        return jnp.concatenate([lines[:capacity, 8 * at : 8 * at + 1] for at in range(n_m)], axis=0)

    def partner(k):
        for h, cols in enumerate(parts):
            landed(piece(k, core_peer, t, cols), CORE_OWN + h, k)
            landed(piece(k, other_x, t, cols), CORE_X + h, k)
        for j in range(1, n_tp):
            for h, cols in enumerate(parts):
                landed(piece(k, core_peer, behind(j), cols), core_y(j) + h, k)
            landed(piece(k, other_x, behind(j), first_cols), core_a(j), k)
            landed(piece(k, other_x, behind(j), last_cols), core_b(j), k)

    def compute(k):
        def part(tp_at, base, size):
            return full[k, :, tp_at, :, base : base + size].reshape(held, size)

        def contract(base, w_ref, nt):
            total = None
            for tp_at in range(n_tp):
                cols = slice(tp_at * share, (tp_at + 1) * share)
                rows = part(tp_at, base, share)
                if nt:
                    term = lax.dot_general(rows, w_ref[0, :, cols], NT, preferred_element_type=F32)
                else:
                    term = jnp.dot(rows, w_ref[0, cols, :], preferred_element_type=F32)
                total = term if total is None else total + term
            return total

        gpre = contract(0, wg_ref, False)
        upre = contract(0, wu_ref, False)
        qvals = contract(share, wd_ref, True)
        lane = lax.broadcasted_iota(jnp.int32, (held, LANES), 1)
        weight = weights(k)
        sig = jax.nn.sigmoid(gpre)
        silu_val = gpre * sig
        hidden = (silu_val * upre).astype(BF16).astype(F32)
        gate_part = jnp.sum(hidden * qvals, axis=1, keepdims=True)
        dhid = weight * qvals
        d_gate = (dhid * upre * sig * (1.0 + gpre * (1.0 - sig))).astype(BF16)
        d_up = (dhid * silu_val).astype(BF16)
        dg_ref[k] = d_gate
        du_ref[k] = d_up
        sc_ref[k] = (weight * hidden).astype(BF16)
        gate_lanes = jnp.where(lane == k, gate_part, 0.0).reshape(n_m, capacity, LANES)
        for at in range(n_m):
            gacc[at % 2, at // 2, :capacity, :] += gate_lanes[at]
        for tp_at in range(n_tp):
            cols = slice(tp_at * share, (tp_at + 1) * share)
            grad = lax.dot_general(d_gate, wg_ref[0, cols, :], NT, preferred_element_type=F32)
            grad = grad + lax.dot_general(d_up, wu_ref[0, cols, :], NT, preferred_element_type=F32)
            grad = grad.astype(BF16).reshape(n_m, capacity, share)
            for at in range(n_m):
                back[k, at % 2, at // 2, tp_at] = grad[at]
        remote(back.at[k, 1 - core], core_in.at[k], R1, k, core_to).start()

    total = experts * held
    tile = min(share, 512)
    per = share // tile

    def weight_grads(at, down):
        cols = slice(at * tile, (at + 1) * tile)
        base = (at % per) * tile + (share if down else 0)
        rows = full[:, :, at // per, :, base : base + tile].reshape(total, tile)

        def units(ref):
            return ref[...].reshape(total, -1)

        if down:
            gd_ref[0, :, cols] = jnp.dot(units(sc_ref).T, rows, preferred_element_type=F32)
        else:
            flipped = rows.T
            gg_ref[0, cols, :] = jnp.dot(flipped, units(dg_ref), preferred_element_type=F32)
            gu_ref[0, cols, :] = jnp.dot(flipped, units(du_ref), preferred_element_type=F32)

    def add(*terms):
        total = terms[0].astype(F32)
        for term in terms[1:]:
            total = total + term.astype(F32)
        return total.astype(BF16)

    x_other = 1 - x_half

    def across_a(k):
        return back.at[k, core, x_other, :, :, low]

    def across_b(k, j):
        return back.at[k, core, :, ahead(j), :, high]

    def reduce_first(k):
        landed(core_in.at[k], R1, k)
        back[k, core] = add(back[k, core], core_in[k])
        remote(across_a(k), xa_in.at[k], R2A, k, x_to).start()
        for j in range(1, n_tp):
            remote(across_b(k, j), yb_in.at[k, j - 1], r2b(j), k, (e, m, ahead(j))).start()

    def onward_a(k, j):
        return back.at[k, core, x_half, ahead(j), :, low]

    def onward_b(k):
        return back.at[k, core, x_other, t, :, high]

    def reduce_second(k):
        landed(xa_in.at[k], R2A, k)
        for j in range(1, n_tp):
            onward_a(k, j)[...] = add(onward_a(k, j)[...], xa_in[k, ahead(j)])
            remote(onward_a(k, j), ya_in.at[k, j - 1], r3a(j), k, (e, m, ahead(j))).start()
        for j in range(1, n_tp):
            landed(yb_in.at[k, j - 1], r2b(j), k)
        onward_b(k)[...] = add(onward_b(k)[...], *[yb_in[k, j - 1, x_other] for j in range(1, n_tp)])
        remote(onward_b(k), xb_in.at[k], R3B, k, x_to).start()

    def mine_back(k):
        return back.at[k, core, x_half, t]

    def reduce_third(k):
        for j in range(1, n_tp):
            landed(ya_in.at[k, j - 1], r3a(j), k)
        landed(xb_in.at[k], R3B, k)
        ref = mine_back(k)
        ref[:, :half] = add(ref[:, :half], xa_in[k, t], *[ya_in[k, j - 1] for j in range(1, n_tp)])
        ref[:, half:] = add(ref[:, half:], xb_in[k], *[yb_in[k, j - 1, x_half] for j in range(1, n_tp)])

        @pl.when(k != e)
        def _():
            ret_copy(k, e).start()

        @pl.when(k == e)
        def _():
            home[e] = ref[...]

    def ret_copy(k, at):
        return pltpu.make_async_remote_copy(
            src_ref=mine_back(k),
            dst_ref=home.at[at],
            send_sem=send_sem.at[RET, k],
            recv_sem=recv_sem.at[RET, at],
            device_id=(k, m, t),
            device_id_type=MESH,
        )

    def send_z(i, carry):
        there = source(jnp.where(i == 1, 1, experts + 1 - i))
        for h in range(2):
            z_copy(there, e, h).start()
        return carry

    def z_copy(there, at, h):
        return pltpu.make_async_remote_copy(
            src_ref=send_ref.at[there, :, parts[h]],
            dst_ref=full.at[at, m, t, :, parts[h]],
            send_sem=send_sem.at[Z + h, there],
            recv_sem=recv_sem.at[Z + h, at],
            device_id=(there, m, t),
            device_id_type=MESH,
        )

    own_here()
    lax.fori_loop(1, experts, send_z, 0)

    def send_weight(d, carry):
        weight_copy(d).start()
        return carry

    lax.fori_loop(1, n_ep, send_weight, 0)

    own(source(1), 0)
    own(source(1), 1)
    neighbours_here()
    neighbours(source(1), 0)
    for load in loads:
        load.wait()

    def step(i, carry):
        at = source(i)
        own(at, 0)
        neighbours(source(i - 1), 1)
        own(at, 1)
        pl.when(i >= 4)(lambda: reduce_first(source(i - 3)))
        pl.when(i >= 5)(lambda: reduce_second(source(i - 4)))
        pl.when(i >= 6)(lambda: reduce_third(source(i - 5)))

        @pl.when(i == 2)
        def _():
            corners_here()
            partner_here()

        @pl.when(i > 2)
        def _():
            corners(source(i - 2))
            partner(source(i - 2))

        compute(source(i - 2))
        neighbours(at, 0)
        return carry

    lax.fori_loop(2, experts, step, 0)

    def reduce(stage, n):
        if n > 0:
            stage(source(n))

    def close(i, carry):
        at = source(i)

        @pl.when(i == experts - 2)
        def _():
            neighbours(source(experts - 1), 1)
            reduce(reduce_first, experts - 3)
            reduce(reduce_second, experts - 4)
            reduce(reduce_third, experts - 5)

        @pl.when(i == experts - 1)
        def _():
            reduce(reduce_second, experts - 3)
            reduce(reduce_third, experts - 4)

        corners(at)
        partner(at)
        pl.when(i == experts - 1)(lambda: reduce_first(source(experts - 2)))
        compute(at)
        return carry

    lax.fori_loop(experts - 2, experts, close, 0)

    def gate_copy(src, dst, n, device):
        return pltpu.make_async_remote_copy(
            src_ref=src,
            dst_ref=dst,
            send_sem=gsend.at[n],
            recv_sem=grecv.at[n],
            device_id=device,
            device_id_type=MESH,
        )

    erows = gcore.shape[2]
    last, second, third = [source(experts - n) for n in (1, 2, 3)]
    rest = [functools.partial(weight_grads, at, down) for at in range(width // tile) for down in (0, 1)]
    early, late = rest[: len(rest) // 3], rest[len(rest) // 3 :]
    middle, late = late[: len(rest) // 4], late[len(rest) // 4 :]
    for at in range(n_m):
        gcore[at % 2, at // 2] = gacc[at % 2, at // 2].T[:erows]
    to_core = gate_copy(gcore.at[1 - core], gcore_in, 0, core_to)
    to_core.start()
    reduce_second(second)
    reduce_third(third)
    reduce_first(last)
    reduce_first(e)
    to_core.wait_recv()
    gcore[core] = gcore[core] + gcore_in[...]
    to_x = gate_copy(gcore.at[core, x_other], gx_in, 1, x_to)
    to_x.start()
    reduce_third(second)
    for part in early:
        part()
    reduce_second(last)
    to_x.wait_recv()
    gt[t] = gcore[core, x_half] + gx_in[...]
    to_t = [gate_copy(gt.at[t], gt.at[t], 1 + j, (e, m, ahead(j))) for j in range(1, n_tp)]
    for copy in to_t:
        copy.start()
    reduce_second(e)
    for part in middle:
        part()
    reduce_third(last)
    reduce_third(e)
    for j in range(1, n_tp):
        gate_copy(gt.at[behind(j)], gt.at[behind(j)], 1 + j, (e, m, ahead(j))).wait_recv()
    whole = gt[0]
    for j in range(1, n_tp):
        whole = whole + gt[j]
    gz[e] = whole
    to_z = [
        gate_copy(gz.at[e], gz.at[e], n_tp + k, (lax.rem(e + k, experts), m, t)) for k in range(1, experts)
    ]
    for copy in to_z:
        copy.start()
    for part in late:
        part()
    for k in range(1, experts):
        src = gz.at[lax.rem(e + experts - k, experts)]
        gate_copy(src, src, n_tp + k, core_to).wait_recv()

    HIGHEST = lax.Precision.HIGHEST
    gates = []
    row = lax.broadcasted_iota(jnp.int32, gz.shape[1:], 0)
    for at in range(experts):
        line = jnp.sum(jnp.where(row == e, gz[at], 0.0), axis=0, keepdims=True)
        line = jnp.broadcast_to(line, (8, LANES))[:, :capacity]
        got = jnp.dot(line, place[at].astype(F32), precision=HIGHEST, preferred_element_type=F32)
        gates.append(got[0:1])
    gate = [sum(picks[n][at] * gates[at] for at in range(experts)) for n in range(TOP)]
    delta = first * (1.0 - first) * (gate[0] - gate[1])
    gate_ref[0:1] = gate[0]
    gate_ref[1:2] = gate[1]
    dlog = jnp.concatenate([delta * (picks[0][at] - picks[1][at]) for at in range(experts)] + blank, axis=0)
    term = jnp.dot(dlog, tok_ref[...].astype(F32), precision=HIGHEST, preferred_element_type=F32)
    cols = width // n_ep
    for at in range(n_ep):
        terms[at, :, :cols] = term[:, at * cols : (at + 1) * cols]

    def term_copy(d):
        there = lax.rem(me + d, n_ep)
        return pltpu.make_async_remote_copy(
            src_ref=terms.at[there],
            dst_ref=terms_in.at[d],
            send_sem=tsend.at[d],
            recv_sem=trecv.at[d],
            device_id=ep_at(d),
            device_id_type=MESH,
        )

    def each(d, carry):
        term_copy(d).start()
        return carry

    lax.fori_loop(1, n_ep, each, 0)

    weight_rows = [rw_ref[:, mine_cols].astype(F32)] + ([jnp.zeros((pad, share), F32)] if pad else [])
    router_part = lax.dot_general(
        dlog, jnp.concatenate(weight_rows, axis=0), (((0,), (0,)), ((), ())), precision=HIGHEST, preferred_element_type=F32
    )
    spread = place[...].reshape(experts * capacity, ntok).T
    for k in range(1, experts):
        at = lax.rem(e + k, experts)
        ret_copy(at, at).wait_recv()
    route_sum = jnp.dot(spread, home[...].reshape(experts * capacity, share), preferred_element_type=F32)
    grad_ref[...] = (route_sum + router_part).astype(BF16)

    def gather(d, total):
        term_copy(d).wait_recv()
        return total + terms_in[d, :, :cols]

    router_ref[...] = lax.fori_loop(1, n_ep, gather, terms[me, :, :cols])[:experts]

    def done(d, carry):
        term_copy(d).wait_send()
        weight_copy(d).wait_send()
        return carry

    lax.fori_loop(1, n_ep, done, 0)
    for copy in [to_core, to_x] + to_t + to_z:
        copy.wait_send()

    def finish(k, carry):
        mine = piece(k, m, t)

        @pl.when(k != e)
        def _():
            sent(mine_back(k), RET, k)
            for h, cols in enumerate(parts):
                mine_part = piece(k, m, t, cols)
                sent(mine_part, Z + h, k)
                sent(mine_part, X + h, k)
                sent(mine_part, CORE_OWN + h, k)
                sent(mine_part, CORE_X + h, k)
                for j in range(1, n_tp):
                    sent(mine_part, y_kind(j) + h, k)
                    sent(mine_part, core_y(j) + h, k)
            for j in range(1, n_tp):
                for kind in (a_kind, b_kind, core_a, core_b):
                    sent(piece(k, m, t, first_cols), kind(j), k)

        @pl.when(k == e)
        def _():
            sent(mine, X, e)
            sent(full.at[e, m], CORE_OWN, e)
            sent(mine, CORE_X, e)
            for j in range(1, n_tp):
                for kind in (a_kind, b_kind, core_a, core_b):
                    sent(piece(e, m, t, first_cols), kind(j), e)

        sent(core_in.at[k], R1, k)
        sent(across_a(k), R2A, k)
        sent(onward_b(k), R3B, k)
        for j in range(1, n_tp):
            sent(across_b(k, j), r2b(j), k)
            sent(onward_a(k, j), r3a(j), k)
        return carry

    lax.fori_loop(0, experts, finish, 0)


def hand_over(*refs):
    n = len(refs) // 2
    copies = [
        pltpu.make_async_copy(src, dst, refs[-1].at[at])
        for at, (src, dst) in enumerate(zip(refs[:n], refs[n:-1]))
    ]
    for copy in copies:
        copy.start()
    for copy in copies:
        copy.wait()


def shards(tokens, routes, router_weight, gate_proj, up_proj, down_proj, cotangent):
    ntok, width = tokens.shape
    experts = router_weight.shape[1]
    n_m, n_tp = lax.axis_size("m"), lax.axis_size("tp")
    share = width // n_tp
    capacity = min(ntok, 5 * TOP * ntok // (4 * experts))
    capacity = -(-capacity // 16) * 16
    ff = gate_proj.shape[2]

    wide = 2 * share
    held = n_m * capacity
    hid_shape = jax.ShapeDtypeStruct((experts, held, ff), BF16)
    flops = 2 * experts * held * width * ff
    kinds = 12 + 10 * (n_tp - 1)
    n_ep = experts * n_m
    half = share // 2
    erows = -(-experts // 8) * 8
    cols = width // n_ep
    vmem = pl.BlockSpec(memory_space=pltpu.VMEM)
    anywhere = pl.BlockSpec(memory_space=pl.ANY)
    full_shape = (experts, n_m, n_tp, capacity, wide)
    grad_gate, grad_up, grad_down, token_grad, gate_rows, router_rows = pl.pallas_call(
        functools.partial(rows_kernel, share),
        in_specs=[vmem] * 4 + [anywhere] * 3,
        out_specs=[vmem] * 6,
        out_shape=[
            pltpu.VMEM(gate_proj.shape, F32),
            pltpu.VMEM(up_proj.shape, F32),
            pltpu.VMEM(down_proj.shape, F32),
            pltpu.VMEM((ntok, share), BF16),
            pltpu.VMEM((TOP, ntok), F32),
            pltpu.VMEM((experts, cols), F32),
        ],
        scratch_shapes=[
            pltpu.VMEM((experts, capacity, wide), BF16),
            pltpu.VMEM((experts, 8, LANES), F32),
            pltpu.VMEM((n_ep, 8, LANES), F32),
            pltpu.VMEM(full_shape, BF16),
            pltpu.VMEM(gate_proj.shape, BF16),
            pltpu.VMEM(up_proj.shape, BF16),
            pltpu.VMEM(down_proj.shape, BF16),
            pltpu.VMEM(hid_shape.shape, BF16),
            pltpu.VMEM(hid_shape.shape, BF16),
            pltpu.VMEM(hid_shape.shape, BF16),
            pltpu.VMEM((experts, 2, 2, n_tp, capacity, share), BF16),
            pltpu.VMEM((experts, 2, n_tp, capacity, share), BF16),
            pltpu.VMEM((experts, n_tp, capacity, half), BF16),
            pltpu.VMEM((experts, n_tp - 1, 2, capacity, share - half), BF16),
            pltpu.VMEM((experts, n_tp - 1, capacity, half), BF16),
            pltpu.VMEM((experts, capacity, share - half), BF16),
            pltpu.VMEM((experts, capacity, share), BF16),
            pltpu.VMEM((experts, capacity, ntok), BF16),
            pltpu.VMEM((2, 2, LANES, LANES), F32),
            pltpu.VMEM((2, 2, erows, LANES), F32),
            pltpu.VMEM((2, erows, LANES), F32),
            pltpu.VMEM((erows, LANES), F32),
            pltpu.VMEM((n_tp, erows, LANES), F32),
            pltpu.VMEM((experts, erows, LANES), F32),
            pltpu.VMEM((n_ep, erows, LANES), F32),
            pltpu.VMEM((n_ep, erows, LANES), F32),
            pltpu.SemaphoreType.DMA((kinds, experts)),
            pltpu.SemaphoreType.DMA((kinds, experts)),
            pltpu.SemaphoreType.DMA((4,)),
            pltpu.SemaphoreType.DMA((n_tp + experts,)),
            pltpu.SemaphoreType.DMA((n_tp + experts,)),
            pltpu.SemaphoreType.DMA((n_ep,)),
            pltpu.SemaphoreType.DMA((n_ep,)),
            pltpu.SemaphoreType.DMA((n_ep,)),
            pltpu.SemaphoreType.DMA((n_ep,)),
        ],
        compiler_params=pltpu.CompilerParams(
            collective_id=0, has_side_effects=True, vmem_limit_bytes=46 << 20
        ),
        cost_estimate=pl.CostEstimate(flops=5 * flops, bytes_accessed=30 << 20, transcendentals=0),
        name="rows",
    )(
        tokens,
        cotangent,
        routes.T,
        router_weight.T,
        gate_proj,
        up_proj,
        down_proj,
    )

    results = (grad_gate, grad_up, grad_down, token_grad, gate_rows, router_rows)
    grad_gate, grad_up, grad_down, token_grad, gate_rows, router_rows = pl.pallas_call(
        hand_over,
        in_specs=[vmem] * 6,
        out_specs=[anywhere] * 6,
        out_shape=[jax.ShapeDtypeStruct(at.shape, at.dtype) for at in results],
        scratch_shapes=[pltpu.SemaphoreType.DMA((6,))],
        compiler_params=pltpu.CompilerParams(vmem_limit_bytes=1 << 20),
        name="hand_over",
    )(*results)
    return (token_grad, gate_rows.T, router_rows.T, grad_gate, grad_up, grad_down)


def solution(mesh):
    devices = mesh.devices
    grid = Mesh(
        devices.reshape(devices.shape[0] // MEMBERS, MEMBERS, devices.shape[1]), ("e", "m", "tp")
    )
    ep = ("e", "m")
    return jax.shard_map(
        shards,
        mesh=grid,
        in_specs=(
            P(ep, None),
            P(ep, None),
            P(),
            P(ep, None, "tp"),
            P(ep, None, "tp"),
            P(ep, "tp", None),
            P(ep, None),
        ),
        out_specs=(
            P(ep, "tp"),
            P(ep, None),
            P(ep, None),
            P(ep, None, "tp"),
            P(ep, None, "tp"),
            P(ep, "tp", None),
        ),
        check_vma=False,
    )
```

```python
import functools

import jax
import jax.numpy as jnp
from jax import lax
from jax.experimental import pallas as pl
from jax.experimental.pallas import tpu as pltpu
from jax.sharding import Mesh, PartitionSpec as P

MEMBERS = 4
TOP = 2
LANES = 128
F32 = jnp.float32
BF16 = jnp.bfloat16
MESH = pl.DeviceIdType.MESH
NT = (((1,), (1,)), ((), ()))


def rows_kernel(
    share, tok_ref, cot_ref, route_ref, rw_ref, wg_hbm, wu_hbm, wd_hbm,
    gg_ref, gu_ref, gd_ref, grad_ref, gate_ref, router_ref,
    send_ref, gw, gw_in, full, wg_ref, wu_ref, wd_ref, dg_ref, du_ref, sc_ref, back, core_in, xa_in, yb_in, ya_in, xb_in, home, place,
    gacc, gcore, gcore_in, gx_in, gt, gz, terms, terms_in,
    send_sem, recv_sem, load_sem, gsend, grecv, tsend, trecv, wsend, wrecv,
):
    experts, n_m, n_tp, capacity, _ = full.shape
    ntok, width = tok_ref.shape
    half = share // 2
    e, m, t = lax.axis_index("e"), lax.axis_index("m"), lax.axis_index("tp")
    n_ep = experts * n_m
    me = e * n_m + m
    x_half, core = lax.div(m, 2), lax.rem(m, 2)
    x_peer = lax.rem(m + 2, 4)
    core_peer = m + 1 - 2 * core
    held = n_m * capacity
    first_cols, last_cols = pl.ds(0, share), pl.ds(share, share)
    low, high = pl.ds(0, half), pl.ds(half, share - half)

    def ahead(j):
        return lax.rem(t + j, n_tp)

    def behind(j):
        return lax.rem(t + n_tp - j, n_tp)

    def ep_at(d):
        there = lax.rem(me + d, n_ep)
        return (lax.div(there, n_m), lax.rem(there, n_m), t)

    barrier = pltpu.get_barrier_semaphore()
    for d in range(1, n_ep):
        pl.semaphore_signal(barrier, inc=1, device_id=ep_at(d), device_id_type=MESH)
    for j in range(1, n_tp):
        pl.semaphore_signal(barrier, inc=1, device_id=(e, m, ahead(j)), device_id_type=MESH)
    loads = [
        pltpu.make_async_copy(src, dst, load_sem.at[n])
        for n, (src, dst) in enumerate([(wg_hbm, wg_ref), (wu_hbm, wu_ref), (wd_hbm, wd_ref)])
    ]
    for load in loads:
        load.start()

    logits = lax.dot_general(rw_ref[...], tok_ref[...], NT, preferred_element_type=F32)
    picks = [
        [jnp.where(route_ref[n : n + 1, :] == at, 1.0, 0.0) for at in range(experts)] for n in range(TOP)
    ]
    chosen = [sum(picks[n][at] * logits[at : at + 1] for at in range(experts)) for n in range(TOP)]
    first = jax.nn.sigmoid(chosen[0] - chosen[1])
    used = [gate.astype(BF16).astype(F32) for gate in (first, 1.0 - first)]
    pad = -experts % 8
    blank = [jnp.zeros((pad, ntok), F32)] if pad else []
    named = jnp.concatenate([picks[0][at] + picks[1][at] for at in range(experts)] + blank, axis=0)
    order = lax.broadcasted_iota(jnp.int32, (ntok, ntok), 0) < lax.broadcasted_iota(jnp.int32, (ntok, ntok), 1)
    rank = jnp.dot(named.astype(BF16), jnp.where(order, 1.0, 0.0).astype(BF16), preferred_element_type=F32)
    slot = jnp.where(named > 0.0, rank, -1.0).astype(jnp.int32)
    line = lax.broadcasted_iota(jnp.int32, (capacity, ntok), 0)
    for at in range(experts):
        chosen_slot = jnp.where(line == slot[at : at + 1], 1.0, 0.0)
        place[at] = chosen_slot.astype(BF16)
        gate_row = (picks[0][at] * used[0] + picks[1][at] * used[1]).astype(BF16)
        gw[at, :, :capacity] = lax.dot_general(
            jnp.broadcast_to(gate_row, (8, ntok)), place[at], NT, preferred_element_type=F32
        )
    gw_in[me] = gw[e]
    mine_cols = pl.ds(pl.multiple_of(t * share, LANES), share)
    spots = place[...].reshape(experts * capacity, ntok)
    for n, ref in enumerate((tok_ref, cot_ref)):
        rows = jnp.dot(spots, ref[:, mine_cols], preferred_element_type=F32).astype(BF16)
        send_ref[:, :, n * share : (n + 1) * share] = rows.reshape(experts, capacity, share)
    for tp_at in range(n_tp):
        cols = slice(tp_at * share, (tp_at + 1) * share)
        for n, ref in enumerate((tok_ref, cot_ref)):
            rows = jnp.dot(place[e], ref[:, cols], preferred_element_type=F32)
            full[e, m, tp_at, :, n * share : (n + 1) * share] = rows.astype(BF16)
    gacc[...] = jnp.zeros_like(gacc)
    pl.semaphore_wait(barrier, n_ep - 1 + n_tp - 1)

    near = lax.min(e, experts - 1 - e)
    side = 1 - 2 * lax.div(2 * e, experts)

    def source(i):
        step, both = lax.div(i + 1, 2), i <= 2 * near
        away = jnp.where(both, step, i - near)
        return e + side * jnp.where(both & (lax.rem(i, 2) == 0), -away, away)

    def remote(src, dst, kind, k, device):
        return pltpu.make_async_remote_copy(
            src_ref=src,
            dst_ref=dst,
            send_sem=send_sem.at[kind, k],
            recv_sem=recv_sem.at[kind, k],
            device_id=device,
            device_id_type=MESH,
        )

    def piece(k, src_m, src_t, cols=None):
        ref = full.at[k, src_m, src_t]
        return ref if cols is None else ref.at[:, cols]

    others = n_tp - 1
    X, CORE_OWN, CORE_X, Z, R1, R2A, R3B, RET = 0, 2, 4, 6, 8, 9, 10, 11
    def y_kind(j): return 12 + 2 * (j - 1)
    def core_y(j): return 12 + 2 * others + 2 * (j - 1)
    def a_kind(j): return 12 + 4 * others + (j - 1)
    def b_kind(j): return 12 + 5 * others + (j - 1)
    def core_a(j): return 12 + 6 * others + (j - 1)
    def core_b(j): return 12 + 7 * others + (j - 1)
    def r2b(j): return 12 + 8 * others + (j - 1)
    def r3a(j): return 12 + 9 * others + (j - 1)

    parts = (first_cols, last_cols)

    x_to, core_to = (e, x_peer, t), (e, core_peer, t)

    def pass_on(ref, kind, k, device):
        remote(ref, ref, kind, k, device).start()

    def landed(ref, kind, k):
        remote(ref, ref, kind, k, core_to).wait_recv()

    def sent(ref, kind, k):
        remote(ref, ref, kind, k, core_to).wait_send()

    def own(k, h):
        mine = piece(k, m, t, parts[h])
        landed(mine, Z + h, k)
        pass_on(mine, X + h, k, x_to)
        for j in range(1, n_tp):
            pass_on(mine, y_kind(j) + h, k, (e, m, ahead(j)))
        pass_on(mine, CORE_OWN + h, k, core_to)

    def neighbours(k, h):
        across = piece(k, x_peer, t, parts[h])

        def along_y():
            for j in range(1, n_tp):
                beside = piece(k, m, behind(j), parts[h])
                landed(beside, y_kind(j) + h, k)
                if h == 0:
                    pass_on(beside, a_kind(j), k, x_to)
                pass_on(beside, core_y(j) + h, k, core_to)

        if h == 0:
            along_y()
        landed(across, X + h, k)
        if h == 1:
            for j in range(1, n_tp):
                pass_on(across, b_kind(j), k, (e, m, ahead(j)))
        pass_on(across, CORE_X + h, k, core_to)
        if h == 1:
            along_y()

    def corners(k):
        for j in range(1, n_tp):
            for cols, kind, across in ((first_cols, a_kind, core_a), (last_cols, b_kind, core_b)):
                ref = piece(k, x_peer, behind(j), cols)
                landed(ref, kind(j), k)
                pass_on(ref, across(j), k, core_to)

    def own_here():
        pass_on(piece(e, m, t), X, e, x_to)
        for j in range(1, n_tp):
            pass_on(piece(e, m, ahead(j), first_cols), a_kind(j), e, x_to)
        pass_on(full.at[e, m], CORE_OWN, e, core_to)

    def neighbours_here():
        across = piece(e, x_peer, t)
        landed(across, X, e)
        for j in range(1, n_tp):
            pass_on(piece(e, x_peer, t, last_cols), b_kind(j), e, (e, m, ahead(j)))
        pass_on(across, CORE_X, e, core_to)

    def corners_here():
        for j in range(1, n_tp):
            ref = piece(e, x_peer, ahead(j), first_cols)
            landed(ref, a_kind(j), e)
            pass_on(ref, core_a(j), e, core_to)
            ref = piece(e, x_peer, behind(j), last_cols)
            landed(ref, b_kind(j), e)
            pass_on(ref, core_b(j), e, core_to)

    other_x = lax.rem(core_peer + 2, 4)

    def partner_here():
        landed(full.at[e, core_peer], CORE_OWN, e)
        landed(piece(e, other_x, t), CORE_X, e)
        for j in range(1, n_tp):
            landed(piece(e, other_x, ahead(j), first_cols), core_a(j), e)
            landed(piece(e, other_x, behind(j), last_cols), core_b(j), e)

    def weight_copy(d):
        there = ep_at(d)
        return pltpu.make_async_remote_copy(
            src_ref=gw.at[there[0]],
            dst_ref=gw_in.at[me],
            send_sem=wsend.at[d],
            recv_sem=wrecv.at[d],
            device_id=there,
            device_id_type=MESH,
        )

    def weights(k):
        for at in range(n_m):
            d = lax.rem(me + n_ep - k * n_m - at, n_ep)
            pl.when(d > 0)(lambda d=d: weight_copy(d).wait_recv())
        lines = gw_in[pl.ds(k * n_m, n_m)].reshape(n_m * 8, LANES).T
        return jnp.concatenate([lines[:capacity, 8 * at : 8 * at + 1] for at in range(n_m)], axis=0)

    def partner(k):
        for h, cols in enumerate(parts):
            landed(piece(k, core_peer, t, cols), CORE_OWN + h, k)
            landed(piece(k, other_x, t, cols), CORE_X + h, k)
        for j in range(1, n_tp):
            for h, cols in enumerate(parts):
                landed(piece(k, core_peer, behind(j), cols), core_y(j) + h, k)
            landed(piece(k, other_x, behind(j), first_cols), core_a(j), k)
            landed(piece(k, other_x, behind(j), last_cols), core_b(j), k)

    def compute(k):
        def part(tp_at, base, size):
            return full[k, :, tp_at, :, base : base + size].reshape(held, size)

        def contract(base, w_ref, nt):
            total = None
            for tp_at in range(n_tp):
                cols = slice(tp_at * share, (tp_at + 1) * share)
                rows = part(tp_at, base, share)
                if nt:
                    term = lax.dot_general(rows, w_ref[0, :, cols], NT, preferred_element_type=F32)
                else:
                    term = jnp.dot(rows, w_ref[0, cols, :], preferred_element_type=F32)
                total = term if total is None else total + term
            return total

        gpre = contract(0, wg_ref, False)
        upre = contract(0, wu_ref, False)
        qvals = contract(share, wd_ref, True)
        lane = lax.broadcasted_iota(jnp.int32, (held, LANES), 1)
        weight = weights(k)
        sig = jax.nn.sigmoid(gpre)
        silu_val = gpre * sig
        hidden = (silu_val * upre).astype(BF16).astype(F32)
        gate_part = jnp.sum(hidden * qvals, axis=1, keepdims=True)
        dhid = weight * qvals
        d_gate = (dhid * upre * sig * (1.0 + gpre * (1.0 - sig))).astype(BF16)
        d_up = (dhid * silu_val).astype(BF16)
        dg_ref[k] = d_gate
        du_ref[k] = d_up
        sc_ref[k] = (weight * hidden).astype(BF16)
        gate_lanes = jnp.where(lane == k, gate_part, 0.0).reshape(n_m, capacity, LANES)
        for at in range(n_m):
            gacc[at % 2, at // 2, :capacity, :] += gate_lanes[at]
        for tp_at in range(n_tp):
            cols = slice(tp_at * share, (tp_at + 1) * share)
            grad = lax.dot_general(d_gate, wg_ref[0, cols, :], NT, preferred_element_type=F32)
            grad = grad + lax.dot_general(d_up, wu_ref[0, cols, :], NT, preferred_element_type=F32)
            grad = grad.astype(BF16).reshape(n_m, capacity, share)
            for at in range(n_m):
                back[k, at % 2, at // 2, tp_at] = grad[at]
        remote(back.at[k, 1 - core], core_in.at[k], R1, k, core_to).start()

    total = experts * held
    tile = min(share, 512)
    per = share // tile

    def weight_grads(at, down):
        cols = slice(at * tile, (at + 1) * tile)
        base = (at % per) * tile + (share if down else 0)
        rows = full[:, :, at // per, :, base : base + tile].reshape(total, tile)

        def units(ref):
            return ref[...].reshape(total, -1)

        if down:
            gd_ref[0, :, cols] = jnp.dot(units(sc_ref).T, rows, preferred_element_type=F32)
        else:
            flipped = rows.T
            gg_ref[0, cols, :] = jnp.dot(flipped, units(dg_ref), preferred_element_type=F32)
            gu_ref[0, cols, :] = jnp.dot(flipped, units(du_ref), preferred_element_type=F32)

    def add(*terms):
        total = terms[0].astype(F32)
        for term in terms[1:]:
            total = total + term.astype(F32)
        return total.astype(BF16)

    x_other = 1 - x_half

    def across_a(k):
        return back.at[k, core, x_other, :, :, low]

    def across_b(k, j):
        return back.at[k, core, :, ahead(j), :, high]

    def reduce_first(k):
        landed(core_in.at[k], R1, k)
        back[k, core] = add(back[k, core], core_in[k])
        remote(across_a(k), xa_in.at[k], R2A, k, x_to).start()
        for j in range(1, n_tp):
            remote(across_b(k, j), yb_in.at[k, j - 1], r2b(j), k, (e, m, ahead(j))).start()

    def onward_a(k, j):
        return back.at[k, core, x_half, ahead(j), :, low]

    def onward_b(k):
        return back.at[k, core, x_other, t, :, high]

    def reduce_second(k):
        landed(xa_in.at[k], R2A, k)
        for j in range(1, n_tp):
            onward_a(k, j)[...] = add(onward_a(k, j)[...], xa_in[k, ahead(j)])
            remote(onward_a(k, j), ya_in.at[k, j - 1], r3a(j), k, (e, m, ahead(j))).start()
        for j in range(1, n_tp):
            landed(yb_in.at[k, j - 1], r2b(j), k)
        onward_b(k)[...] = add(onward_b(k)[...], *[yb_in[k, j - 1, x_other] for j in range(1, n_tp)])
        remote(onward_b(k), xb_in.at[k], R3B, k, x_to).start()

    def mine_back(k):
        return back.at[k, core, x_half, t]

    def reduce_third(k):
        for j in range(1, n_tp):
            landed(ya_in.at[k, j - 1], r3a(j), k)
        landed(xb_in.at[k], R3B, k)
        ref = mine_back(k)
        ref[:, :half] = add(ref[:, :half], xa_in[k, t], *[ya_in[k, j - 1] for j in range(1, n_tp)])
        ref[:, half:] = add(ref[:, half:], xb_in[k], *[yb_in[k, j - 1, x_half] for j in range(1, n_tp)])

        @pl.when(k != e)
        def _():
            ret_copy(k, e).start()

        @pl.when(k == e)
        def _():
            home[e] = ref[...]

    def ret_copy(k, at):
        return pltpu.make_async_remote_copy(
            src_ref=mine_back(k),
            dst_ref=home.at[at],
            send_sem=send_sem.at[RET, k],
            recv_sem=recv_sem.at[RET, at],
            device_id=(k, m, t),
            device_id_type=MESH,
        )

    def send_z(i, carry):
        there = source(jnp.where(i == 1, 1, experts + 1 - i))

        for h in range(2):
            z_copy(there, e, h).start()
        return carry

    def z_copy(there, at, h):
        return pltpu.make_async_remote_copy(
            src_ref=send_ref.at[there, :, parts[h]],
            dst_ref=full.at[at, m, t, :, parts[h]],
            send_sem=send_sem.at[Z + h, there],
            recv_sem=recv_sem.at[Z + h, at],
            device_id=(there, m, t),
            device_id_type=MESH,
        )

    def send_far():
        lax.fori_loop(2, experts, send_z, 0)

    own_here()
    send_z(1, 0)
    pl.when(near > 0)(send_far)

    def send_weight(d, carry):
        weight_copy(d).start()
        return carry

    lax.fori_loop(1, n_ep, send_weight, 0)

    own(source(1), 0)
    own(source(1), 1)
    neighbours_here()
    neighbours(source(1), 0)
    pl.when(near == 0)(send_far)
    neighbours(source(1), 1)
    for load in loads:
        load.wait()

    def step(i, carry):
        at = source(i)
        own(at, 0)
        pl.when(i > 2)(lambda: neighbours(source(i - 1), 1))
        own(at, 1)
        pl.when(i >= 4)(lambda: reduce_first(source(i - 3)))
        pl.when(i >= 5)(lambda: reduce_second(source(i - 4)))
        pl.when(i >= 6)(lambda: reduce_third(source(i - 5)))

        @pl.when(i == 2)
        def _():
            corners_here()
            partner_here()

        @pl.when(i > 2)
        def _():
            corners(source(i - 2))
            partner(source(i - 2))

        compute(source(i - 2))
        neighbours(at, 0)
        return carry

    lax.fori_loop(2, experts, step, 0)

    def reduce(stage, n):
        if n > 0:
            stage(source(n))

    def close(i, carry):
        at = source(i)

        @pl.when(i == experts - 2)
        def _():
            neighbours(source(experts - 1), 1)
            reduce(reduce_first, experts - 3)
            reduce(reduce_second, experts - 4)
            reduce(reduce_third, experts - 5)

        @pl.when(i == experts - 1)
        def _():
            reduce(reduce_second, experts - 3)
            reduce(reduce_third, experts - 4)

        corners(at)
        partner(at)
        pl.when(i == experts - 1)(lambda: reduce_first(source(experts - 2)))
        compute(at)
        return carry

    lax.fori_loop(experts - 2, experts, close, 0)

    def gate_copy(src, dst, n, device):
        return pltpu.make_async_remote_copy(
            src_ref=src,
            dst_ref=dst,
            send_sem=gsend.at[n],
            recv_sem=grecv.at[n],
            device_id=device,
            device_id_type=MESH,
        )

    erows = gcore.shape[2]
    last, second, third = [source(experts - n) for n in (1, 2, 3)]
    rest = [functools.partial(weight_grads, at, down) for at in range(width // tile) for down in (0, 1)]
    early, late = rest[: len(rest) // 3], rest[len(rest) // 3 :]
    middle, late = late[: len(rest) // 4], late[len(rest) // 4 :]
    for at in range(n_m):
        gcore[at % 2, at // 2] = gacc[at % 2, at // 2].T[:erows]
    to_core = gate_copy(gcore.at[1 - core], gcore_in, 0, core_to)
    to_core.start()
    reduce_second(second)
    reduce_third(third)
    reduce_first(last)
    to_core.wait_recv()
    gcore[core] = gcore[core] + gcore_in[...]
    to_x = gate_copy(gcore.at[core, x_other], gx_in, 1, x_to)
    to_x.start()
    reduce_third(second)
    reduce_first(e)
    for part in early:
        part()
    reduce_second(last)
    to_x.wait_recv()
    gt[t] = gcore[core, x_half] + gx_in[...]
    to_t = [gate_copy(gt.at[t], gt.at[t], 1 + j, (e, m, ahead(j))) for j in range(1, n_tp)]
    for copy in to_t:
        copy.start()
    reduce_second(e)
    for part in middle:
        part()
    reduce_third(last)
    reduce_third(e)
    for j in range(1, n_tp):
        gate_copy(gt.at[behind(j)], gt.at[behind(j)], 1 + j, (e, m, ahead(j))).wait_recv()
    whole = gt[0]
    for j in range(1, n_tp):
        whole = whole + gt[j]
    gz[e] = whole
    to_z = [
        gate_copy(gz.at[e], gz.at[e], n_tp + k, (lax.rem(e + k, experts), m, t)) for k in range(1, experts)
    ]
    for copy in to_z:
        copy.start()
    for k in range(1, experts):
        src = gz.at[lax.rem(e + experts - k, experts)]
        gate_copy(src, src, n_tp + k, core_to).wait_recv()

    HIGHEST = lax.Precision.HIGHEST
    gates = []
    row = lax.broadcasted_iota(jnp.int32, gz.shape[1:], 0)
    for at in range(experts):
        line = jnp.sum(jnp.where(row == e, gz[at], 0.0), axis=0, keepdims=True)
        line = jnp.broadcast_to(line, (8, LANES))[:, :capacity]
        got = jnp.dot(line, place[at].astype(F32), precision=HIGHEST, preferred_element_type=F32)
        gates.append(got[0:1])
    gate = [sum(picks[n][at] * gates[at] for at in range(experts)) for n in range(TOP)]
    delta = first * (1.0 - first) * (gate[0] - gate[1])
    gate_ref[0:1] = gate[0]
    gate_ref[1:2] = gate[1]
    dlog = jnp.concatenate([delta * (picks[0][at] - picks[1][at]) for at in range(experts)] + blank, axis=0)
    term = jnp.dot(dlog, tok_ref[...].astype(F32), precision=HIGHEST, preferred_element_type=F32)
    cols = width // n_ep
    for at in range(n_ep):
        terms[at, :, :cols] = term[:, at * cols : (at + 1) * cols]

    def term_copy(d):
        there = lax.rem(me + d, n_ep)
        return pltpu.make_async_remote_copy(
            src_ref=terms.at[there],
            dst_ref=terms_in.at[d],
            send_sem=tsend.at[d],
            recv_sem=trecv.at[d],
            device_id=ep_at(d),
            device_id_type=MESH,
        )

    def each(d, carry):
        term_copy(d).start()
        return carry

    lax.fori_loop(1, n_ep, each, 0)
    for part in late:
        part()

    weight_rows = [rw_ref[:, mine_cols].astype(F32)] + ([jnp.zeros((pad, share), F32)] if pad else [])
    router_part = lax.dot_general(
        dlog, jnp.concatenate(weight_rows, axis=0), (((0,), (0,)), ((), ())), precision=HIGHEST, preferred_element_type=F32
    )
    spread = place[...].reshape(experts * capacity, ntok).T
    for k in range(1, experts):
        at = lax.rem(e + k, experts)
        ret_copy(at, at).wait_recv()
    route_sum = jnp.dot(spread, home[...].reshape(experts * capacity, share), preferred_element_type=F32)
    grad_ref[...] = (route_sum + router_part).astype(BF16)

    def gather(d, total):
        term_copy(d).wait_recv()
        return total + terms_in[d, :, :cols]

    router_ref[...] = lax.fori_loop(1, n_ep, gather, terms[me, :, :cols])[:experts]

    def done(d, carry):
        term_copy(d).wait_send()
        weight_copy(d).wait_send()
        return carry

    lax.fori_loop(1, n_ep, done, 0)
    for copy in [to_core, to_x] + to_t + to_z:
        copy.wait_send()

    def finish(k, carry):
        mine = piece(k, m, t)

        @pl.when(k != e)
        def _():
            sent(mine_back(k), RET, k)
            for h, cols in enumerate(parts):
                mine_part = piece(k, m, t, cols)
                sent(mine_part, Z + h, k)
                sent(mine_part, X + h, k)
                sent(mine_part, CORE_OWN + h, k)
                sent(mine_part, CORE_X + h, k)
                for j in range(1, n_tp):
                    sent(mine_part, y_kind(j) + h, k)
                    sent(mine_part, core_y(j) + h, k)
            for j in range(1, n_tp):
                for kind in (a_kind, b_kind, core_a, core_b):
                    sent(piece(k, m, t, first_cols), kind(j), k)

        @pl.when(k == e)
        def _():
            sent(mine, X, e)
            sent(full.at[e, m], CORE_OWN, e)
            sent(mine, CORE_X, e)
            for j in range(1, n_tp):
                for kind in (a_kind, b_kind, core_a, core_b):
                    sent(piece(e, m, t, first_cols), kind(j), e)

        sent(core_in.at[k], R1, k)
        sent(across_a(k), R2A, k)
        sent(onward_b(k), R3B, k)
        for j in range(1, n_tp):
            sent(across_b(k, j), r2b(j), k)
            sent(onward_a(k, j), r3a(j), k)
        return carry

    lax.fori_loop(0, experts, finish, 0)


def hand_over(*refs):
    n = len(refs) // 2
    copies = [
        pltpu.make_async_copy(src, dst, refs[-1].at[at])
        for at, (src, dst) in enumerate(zip(refs[:n], refs[n:-1]))
    ]
    for copy in copies:
        copy.start()
    for copy in copies:
        copy.wait()


def shards(tokens, routes, router_weight, gate_proj, up_proj, down_proj, cotangent):
    ntok, width = tokens.shape
    experts = router_weight.shape[1]
    n_m, n_tp = lax.axis_size("m"), lax.axis_size("tp")
    share = width // n_tp
    capacity = min(ntok, 5 * TOP * ntok // (4 * experts))
    capacity = -(-capacity // 16) * 16
    ff = gate_proj.shape[2]

    wide = 2 * share
    held = n_m * capacity
    hid_shape = jax.ShapeDtypeStruct((experts, held, ff), BF16)
    flops = 2 * experts * held * width * ff
    kinds = 12 + 10 * (n_tp - 1)
    n_ep = experts * n_m
    half = share // 2
    erows = -(-experts // 8) * 8
    cols = width // n_ep
    vmem = pl.BlockSpec(memory_space=pltpu.VMEM)
    anywhere = pl.BlockSpec(memory_space=pl.ANY)
    full_shape = (experts, n_m, n_tp, capacity, wide)
    grad_gate, grad_up, grad_down, token_grad, gate_rows, router_rows = pl.pallas_call(
        functools.partial(rows_kernel, share),
        in_specs=[vmem] * 4 + [anywhere] * 3,
        out_specs=[vmem] * 6,
        out_shape=[
            pltpu.VMEM(gate_proj.shape, F32),
            pltpu.VMEM(up_proj.shape, F32),
            pltpu.VMEM(down_proj.shape, F32),
            pltpu.VMEM((ntok, share), BF16),
            pltpu.VMEM((TOP, ntok), F32),
            pltpu.VMEM((experts, cols), F32),
        ],
        scratch_shapes=[
            pltpu.VMEM((experts, capacity, wide), BF16),
            pltpu.VMEM((experts, 8, LANES), F32),
            pltpu.VMEM((n_ep, 8, LANES), F32),
            pltpu.VMEM(full_shape, BF16),
            pltpu.VMEM(gate_proj.shape, BF16),
            pltpu.VMEM(up_proj.shape, BF16),
            pltpu.VMEM(down_proj.shape, BF16),
            pltpu.VMEM(hid_shape.shape, BF16),
            pltpu.VMEM(hid_shape.shape, BF16),
            pltpu.VMEM(hid_shape.shape, BF16),
            pltpu.VMEM((experts, 2, 2, n_tp, capacity, share), BF16),
            pltpu.VMEM((experts, 2, n_tp, capacity, share), BF16),
            pltpu.VMEM((experts, n_tp, capacity, half), BF16),
            pltpu.VMEM((experts, n_tp - 1, 2, capacity, share - half), BF16),
            pltpu.VMEM((experts, n_tp - 1, capacity, half), BF16),
            pltpu.VMEM((experts, capacity, share - half), BF16),
            pltpu.VMEM((experts, capacity, share), BF16),
            pltpu.VMEM((experts, capacity, ntok), BF16),
            pltpu.VMEM((2, 2, LANES, LANES), F32),
            pltpu.VMEM((2, 2, erows, LANES), F32),
            pltpu.VMEM((2, erows, LANES), F32),
            pltpu.VMEM((erows, LANES), F32),
            pltpu.VMEM((n_tp, erows, LANES), F32),
            pltpu.VMEM((experts, erows, LANES), F32),
            pltpu.VMEM((n_ep, erows, LANES), F32),
            pltpu.VMEM((n_ep, erows, LANES), F32),
            pltpu.SemaphoreType.DMA((kinds, experts)),
            pltpu.SemaphoreType.DMA((kinds, experts)),
            pltpu.SemaphoreType.DMA((4,)),
            pltpu.SemaphoreType.DMA((n_tp + experts,)),
            pltpu.SemaphoreType.DMA((n_tp + experts,)),
            pltpu.SemaphoreType.DMA((n_ep,)),
            pltpu.SemaphoreType.DMA((n_ep,)),
            pltpu.SemaphoreType.DMA((n_ep,)),
            pltpu.SemaphoreType.DMA((n_ep,)),
        ],
        compiler_params=pltpu.CompilerParams(
            collective_id=0, has_side_effects=True, vmem_limit_bytes=46 << 20
        ),
        cost_estimate=pl.CostEstimate(flops=5 * flops, bytes_accessed=30 << 20, transcendentals=0),
        name="rows",
    )(
        tokens,
        cotangent,
        routes.T,
        router_weight.T,
        gate_proj,
        up_proj,
        down_proj,
    )

    results = (grad_gate, grad_up, grad_down, token_grad, gate_rows, router_rows)
    grad_gate, grad_up, grad_down, token_grad, gate_rows, router_rows = pl.pallas_call(
        hand_over,
        in_specs=[vmem] * 6,
        out_specs=[anywhere] * 6,
        out_shape=[jax.ShapeDtypeStruct(at.shape, at.dtype) for at in results],
        scratch_shapes=[pltpu.SemaphoreType.DMA((6,))],
        compiler_params=pltpu.CompilerParams(vmem_limit_bytes=1 << 20),
        name="hand_over",
    )(*results)
    return (token_grad, gate_rows.T, router_rows.T, grad_gate, grad_up, grad_down)


def solution(mesh):
    devices = mesh.devices
    grid = Mesh(
        devices.reshape(devices.shape[0] // MEMBERS, MEMBERS, devices.shape[1]), ("e", "m", "tp")
    )
    ep = ("e", "m")
    return jax.shard_map(
        shards,
        mesh=grid,
        in_specs=(
            P(ep, None),
            P(ep, None),
            P(),
            P(ep, None, "tp"),
            P(ep, None, "tp"),
            P(ep, "tp", None),
            P(ep, None),
        ),
        out_specs=(
            P(ep, "tp"),
            P(ep, None),
            P(ep, None),
            P(ep, None, "tp"),
            P(ep, None, "tp"),
            P(ep, "tp", None),
        ),
        check_vma=False,
    )
```
